32 devices in a mesh: ep: 8 (over z, x), tp: 4 (over y, core).
Axes of the slice: x: 2, y: 2, z: 4, core: 2. Of those that a mesh axis runs over, the one named last changes fastest.
Arguments:
- query_logits: bfloat16 [2048, 2048], P('ep', 'tp'), may hold values from -6 to 6
- forget_gate_logits: bfloat16 [2048, 2048], P('ep', 'tp'), may hold values from -3.75 to 3.75
- written_values: bfloat16 [2048, 2048], P('ep', 'tp'), may hold values from -6 to 6
- output_gate_logits: bfloat16 [2048, 2048], P('ep', 'tp'), may hold values from -6 to 6
- gap: float32 [2048], P('tp'), may hold values from 4.8828125e-05 to 0.06
- extra_log_forget: float32 [2048, 2048], P('ep', 'tp'), may hold values from -0.7 to 0
- head_norm_scale: float32 [2048], P('tp'), may hold values from 0.1 to 1.9
- mixer_output_matrix: bfloat16 [2048, 2048], P('tp'), may hold values from -0.125 to 0.125
- expert_input_tokens: bfloat16 [2048, 2048], P('ep'), may hold values from -12 to 12
- expert_norm_scale: float32 [2048], replicated, may hold values from 0.1 to 1.9
- routes: int32 [2048, 2], P('ep'), may hold values from 0 to 7, all different within a row; in each aligned block of 256 rows (0 to 255, 256 to 511, ...) at most 96 rows name the same one
- router_scores_chosen: float32 [2048, 2], P('ep'), may hold values from -6 to 6
- expert_gate_matrix: bfloat16 [8, 2048, 4096], P('ep', None, 'tp'), may hold values from -0.125 to 0.125
- expert_up_matrix: bfloat16 [8, 2048, 4096], P('ep', None, 'tp'), may hold values from -0.125 to 0.125
- expert_down_matrix: bfloat16 [8, 2048, 4096], P('ep', None, 'tp'), may hold values from -0.09375 to 0.09375
Outputs:
- mixer_output_rows: bfloat16 [2048, 2048], P(('ep', 'tp'))
- expert_out: bfloat16 [2048, 2048], P('ep', 'tp')
The draws below stay inside these ranges and needn't reach their ends.
Inputs may be any that keep to these rules, and one draw needn't show every extreme that they name: `routes`: each row names two different experts. Among the rows of one device no expert is named more than 96 times, and 96 is reached in some blocks.
All inputs are finite; a program needn't handle non-finite values.
Results may differ from the reference program's by a relative error of at most 0.019.
Values may be sent and summed in bfloat16 or wider, within the bound.
A program may use at most 64 MiB of HBM per device.

```python
import math
import jax
import jax.numpy as jnp
import numpy as np
from jax import lax

HEAD_DIM = 128
HEADS = 16
D = 2048
FF = 4096
TOK_A = 256
TOK_B = 256
TOKENS_A = 2048
TOKENS_B = 2048
EXPERTS = 8
CAP = 96
N_EP = 8
N_TP = 4


def draw_gap(key, part):
    choose_key, lasting_key, quick_key = jax.random.split(jax.random.fold_in(key, 11), 3)
    quick_heads = jax.random.uniform(choose_key, (HEADS,)) < 0.5
    lasting = jnp.exp(jax.random.uniform(lasting_key, (HEADS, HEAD_DIM), jnp.float32, math.log(0.1 / TOKENS_A), math.log(1.0 / TOKENS_A)))
    quick = jnp.exp(jax.random.uniform(quick_key, (HEADS, HEAD_DIM), jnp.float32, math.log(0.02), math.log(0.06)))
    return jnp.where(quick_heads[:, None], quick, lasting).reshape(D).astype(jnp.float32)


def draw_forget_gate_logits(key, part):
    noise_key, shift_key = jax.random.split(jax.random.fold_in(key, 23), 2)
    block_shift = jax.random.uniform(shift_key, (N_EP,), jnp.float32, -1.2, 1.2)
    noise = jnp.clip(jax.random.normal(noise_key, (TOKENS_A, D), jnp.float32), -2.5, 2.5)
    return (noise + jnp.repeat(block_shift, TOK_A)[:, None]).astype(jnp.bfloat16)


def draw_extra_log_forget(key, part):
    where_key, depth_key = jax.random.split(jax.random.fold_in(key, 37), 2)
    spots = jax.random.randint(where_key, (3,), 0, TOKENS_A)
    struck = jnp.any(jnp.arange(TOKENS_A)[:, None] == spots[None, :], axis=1)
    depth = jnp.log(jax.random.uniform(depth_key, (TOKENS_A, D), jnp.float32, 0.5, 0.8))
    return jnp.where(struck[:, None], depth, 0.0).astype(jnp.float32)


def draw_expert_input_tokens(key, part):
    noise_key, scale_key = jax.random.split(jax.random.fold_in(key, 41), 2)
    scales = jnp.exp(jax.random.uniform(scale_key, (TOKENS_B, 1), jnp.float32, math.log(0.3), math.log(3.0)))
    noise = jnp.clip(jax.random.normal(noise_key, (TOKENS_B, D), jnp.float32), -4.0, 4.0)
    return (noise * scales).astype(jnp.bfloat16)


def block_levels(rng, dims, pieces, least, high):
    gain, own = 1.0, jax.random.fold_in(rng, 6)
    for dim, parts in pieces:
        steps = jnp.exp(jax.random.uniform(jax.random.fold_in(own, dim), (parts,), jnp.float32, least / len(pieces), high / len(pieces)))
        gain = gain * jnp.repeat(steps, dims[dim] // parts).reshape([-1 if axis == dim else 1 for axis in range(len(dims))])
    return gain


def deal_out(rng, own, number, rows, amount, top, most, skew):
    ranking = jax.random.permutation(rng, amount)
    crowded, ordinary = shares(amount, rows * top, most, skew, True), shares(amount, rows * top, most, skew, False)
    places = jnp.arange(amount)

    def named(sizes, offset_by):
        used = int((sizes > 0).sum())
        fixed = max(1, used // 4)
        passed = fixed + (places - fixed + offset_by * (used - fixed)) % max(1, amount - fixed)
        return jnp.zeros((amount,), jnp.int32).at[ranking[jnp.where(places < fixed, places, passed)]].set(jnp.asarray(sizes, jnp.int32))

    sizes = jnp.where(number % 4 == 0, named(crowded, number // 4), named(ordinary, number - number // 4 - 1))
    mixed = jax.random.permutation(jax.random.fold_in(own, 3), amount)
    source_of, taker = mixed[0:amount // 2 * 2:2], mixed[1:amount // 2 * 2:2]
    room = jnp.minimum(sizes[source_of] - 1, most - sizes[taker]) // 2
    room = jnp.where((source_of == ranking[0]) | (taker == ranking[0]) | (sizes[taker] == 0), 0, jnp.maximum(room, 0))
    passed = jax.random.randint(jax.random.fold_in(own, 4), (amount // 2,), 0, 1 << 20) % (room + 1)
    sizes = sizes.at[source_of].add(-passed).at[taker].add(passed)
    members = jnp.searchsorted(jnp.cumsum(sizes), jnp.arange(rows * top), side="right").astype(jnp.int32)
    table = members.reshape(top, rows).T
    table = table[jax.random.permutation(jax.random.fold_in(own, 1), rows)]
    offset_by = jax.random.randint(jax.random.fold_in(own, 2), (rows, 1), 0, top)
    return jnp.take_along_axis(table, (jnp.arange(top)[None, :] + offset_by) % top, axis=1)


def shares(number_of, total, limit, skew, full):
    portions = [(1 << 20) // math.isqrt(standing ** skew) + 1 for standing in range(1, number_of + 1)]
    largest = limit if full else min(limit, max(-(-total // number_of), total * portions[0] // sum(portions)))
    least = 1 if total - largest >= number_of - 1 else 0
    counts, spare = [largest] + [least] * (number_of - 1), total - largest - least * (number_of - 1)
    while spare > 0:
        free = [i for i in range(1, number_of) if counts[i] < largest] or [i for i in range(1, number_of) if counts[i] < limit]
        mass, left = sum([portions[i] for i in free]), spare
        for i in free:
            extra = min(limit - counts[i], max(1, left * portions[i] // mass), spare)
            counts[i] = counts[i] + extra
            spare = spare - extra
    return np.array(counts)


def gaussian(stream_key, shape, deviation, limit, shards=(), kind=jnp.bfloat16):
    loudness = block_levels(stream_key, shape, shards, -0.22, 0.18) if shards else 1.0
    drawn = jax.random.normal(stream_key, shape, jnp.float32) * deviation * loudness
    return jnp.minimum(jnp.maximum(drawn, -limit), limit).astype(kind)


def setup_inputs(seed: int = 0) -> dict:
    streams_of = jax.random.split(jax.random.key(seed), 16)
    query_logits = gaussian(streams_of[0], (TOKENS_A, D), 1.0, 6.0, ((0, 8), (1, 4)))
    forget_gate_logits = draw_forget_gate_logits(jax.random.fold_in(streams_of[15], 71), 0)
    written_values = gaussian(streams_of[2], (TOKENS_A, D), 1.0, 6.0, ((0, 8), (1, 4)))
    output_gate_logits = gaussian(streams_of[3], (TOKENS_A, D), 1.0, 6.0, ((0, 8), (1, 4)))
    gap = draw_gap(jax.random.fold_in(streams_of[15], 71), 0)
    extra_log_forget = draw_extra_log_forget(jax.random.fold_in(streams_of[15], 71), 0)
    head_norm_scale = jnp.clip(1.0 + 0.18 * jax.random.normal(streams_of[6], (D,), jnp.float32), 0.1, 1.9)
    mixer_output_matrix = gaussian(streams_of[7], (D, D), D ** -0.5, 0.125, ((0, 4),))
    expert_input_tokens = draw_expert_input_tokens(jax.random.fold_in(streams_of[15], 71), 0)
    expert_norm_scale = jnp.clip(1.0 + 0.18 * jax.random.normal(streams_of[9], (D,), jnp.float32), 0.1, 1.9)
    routes_keys = jax.random.split(jax.random.fold_in(streams_of[10], 1), TOKENS_B // TOK_B)
    routes_turns = jax.random.permutation(jax.random.fold_in(streams_of[10], 3), TOKENS_B // TOK_B)
    routes = jax.vmap(lambda own, number: deal_out(jax.random.fold_in(streams_of[10], 2), own, number, TOK_B, EXPERTS, 2, CAP, 2))(routes_keys, routes_turns).reshape((TOKENS_B, 2))
    router_scores_chosen = gaussian(streams_of[11], (TOKENS_B, 2), 1.5, 6.0, ((0, 8),), jnp.float32)
    expert_gate_matrix = gaussian(streams_of[12], (EXPERTS, D, FF), D ** -0.5, 0.125, ((0, 8), (2, 4)))
    expert_up_matrix = gaussian(streams_of[13], (EXPERTS, D, FF), D ** -0.5, 0.125, ((0, 8), (2, 4)))
    expert_down_matrix = gaussian(streams_of[14], (EXPERTS, D, FF), FF ** -0.5, 0.09375, ((0, 8), (2, 4)))
    return {"query_logits": query_logits, "forget_gate_logits": forget_gate_logits, "written_values": written_values, "output_gate_logits": output_gate_logits, "gap": gap, "extra_log_forget": extra_log_forget, "head_norm_scale": head_norm_scale, "mixer_output_matrix": mixer_output_matrix, "expert_input_tokens": expert_input_tokens, "expert_norm_scale": expert_norm_scale, "routes": routes, "router_scores_chosen": router_scores_chosen, "expert_gate_matrix": expert_gate_matrix, "expert_up_matrix": expert_up_matrix, "expert_down_matrix": expert_down_matrix}


exact_precision = lax.Precision.HIGHEST

def recurrent_portion(query_logits, forget_gate_logits, written_values, output_gate_logits, gap, extra_log_forget, head_norm_scale, mixer_output_matrix):
    final_result = gap * jax.nn.sigmoid(-forget_gate_logits.astype(jnp.float32))
    decay_logarithm = jnp.log1p(-final_result) + extra_log_forget
    queries = jax.nn.silu(query_logits.astype(jnp.float32))
    values = written_values.astype(jnp.float32)

    def by_head(array):
        return array.reshape(TOKENS_A, HEADS, HEAD_DIM)

    def advance(state, inputs):
        query_now, key_now, value_now, decay_now = inputs
        state = jnp.exp(decay_now)[:, :, None] * state + key_now[:, :, None] * value_now[:, None, :]
        output = jnp.einsum('hd,hdv->hv', query_now, state, precision=exact_precision)
        return (state, output)
    start_state = jnp.zeros((HEADS, HEAD_DIM, HEAD_DIM), jnp.float32)
    _, recurrent = lax.scan(advance, start_state, (by_head(queries), by_head(final_result), by_head(values), by_head(decay_logarithm)))
    scaled = recurrent * lax.rsqrt(lax.optimization_barrier(jnp.mean(recurrent * recurrent, axis=-1, keepdims=True)) + 1e-06)
    scaled = scaled.reshape(TOKENS_A, D)
    hidden = (scaled * head_norm_scale * jax.nn.silu(output_gate_logits.astype(jnp.float32))).astype(jnp.bfloat16)
    group_width = D // N_TP

    def add_group(totals, index):
        columns = lax.dynamic_slice_in_dim(hidden, index * group_width, group_width, 1)
        weight_rows = lax.dynamic_slice_in_dim(mixer_output_matrix, index * group_width, group_width, 0)
        partial_sum = jnp.dot(columns, weight_rows, preferred_element_type=jnp.float32)
        rounded = lax.optimization_barrier(partial_sum.astype(jnp.bfloat16)).astype(jnp.float32)
        return (totals + rounded, None)
    mixed_total, _ = lax.scan(add_group, jnp.zeros((TOKENS_A, D), jnp.float32), jnp.arange(N_TP, dtype=jnp.int32))
    return mixed_total.astype(jnp.bfloat16)

def expert_part(expert_input_tokens, expert_norm_scale, routes, router_scores_chosen, expert_gate_matrix, expert_up_matrix, expert_down_matrix):
    inputs32 = expert_input_tokens.astype(jnp.float32)
    centred = inputs32 - lax.optimization_barrier(jnp.mean(inputs32, axis=-1, keepdims=True))
    variance = lax.optimization_barrier(jnp.mean(centred * centred, axis=-1, keepdims=True))
    normed = (centred * lax.rsqrt(variance + 1e-05) * expert_norm_scale).astype(jnp.bfloat16)
    first_weight = jax.nn.sigmoid(router_scores_chosen[:, 0] - router_scores_chosen[:, 1])
    route_weight = jnp.stack([first_weight, 1.0 - first_weight], axis=1)
    flat_routes = routes.reshape(N_EP, TOK_B * 2)
    onehot = (flat_routes[:, :, None] == jnp.arange(EXPERTS, dtype=jnp.int32)[None, None, :]).astype(jnp.int32)
    earlier = jnp.cumsum(onehot, axis=1) - onehot
    position = lax.optimization_barrier(jnp.sum(earlier * onehot, axis=2))
    slot_count = N_EP * CAP
    source = jnp.arange(N_EP, dtype=jnp.int32)[:, None]
    target = (flat_routes * slot_count + source * CAP + position).reshape(-1).astype(jnp.int32)
    token_ids = jnp.arange(TOKENS_B * 2, dtype=jnp.int32) // 2
    owner = jnp.zeros((EXPERTS * slot_count,), jnp.int32).at[target].set(token_ids)
    filled = jnp.zeros((EXPERTS * slot_count,), jnp.bool_).at[target].set(True)
    group_width = FF // N_TP

    def one_expert(unused, inputs):
        owner_ids, live_slots, gate_w, up_w, down_w = inputs
        picked = jnp.where(live_slots[:, None], normed[owner_ids], jnp.zeros((), jnp.bfloat16))
        gate_act = jnp.dot(picked, gate_w, preferred_element_type=jnp.float32)
        up_act = jnp.dot(picked, up_w, preferred_element_type=jnp.float32)
        hidden = (jax.nn.silu(gate_act) * up_act).astype(jnp.bfloat16)

        def add_group(totals, index):
            hidden_cols = lax.dynamic_slice_in_dim(hidden, index * group_width, group_width, 1)
            down_cols = lax.dynamic_slice_in_dim(down_w, index * group_width, group_width, 1)
            partial_sum = lax.dot_general(hidden_cols, down_cols, (((1,), (1,)), ((), ())), preferred_element_type=jnp.float32)
            rounded = lax.optimization_barrier(partial_sum.astype(jnp.bfloat16)).astype(jnp.float32)
            return (totals + rounded, None)
        summed, _ = lax.scan(add_group, jnp.zeros((slot_count, D), jnp.float32), jnp.arange(N_TP, dtype=jnp.int32))
        return (unused, summed.astype(jnp.bfloat16))
    _, results = lax.scan(one_expert, None, (owner.reshape(EXPERTS, slot_count), filled.reshape(EXPERTS, slot_count), expert_gate_matrix, expert_up_matrix, expert_down_matrix))
    chosen = results.reshape(EXPERTS * slot_count, D)[target].astype(jnp.float32).reshape(TOKENS_B, 2, D)
    return lax.optimization_barrier(jnp.sum(chosen * route_weight[:, :, None], axis=1)).astype(jnp.bfloat16)

def reference(query_logits, forget_gate_logits, written_values, output_gate_logits, gap, extra_log_forget, head_norm_scale, mixer_output_matrix, expert_input_tokens, expert_norm_scale, routes, router_scores_chosen, expert_gate_matrix, expert_up_matrix, expert_down_matrix):
    mixer_output_rows = recurrent_portion(query_logits, forget_gate_logits, written_values, output_gate_logits, gap, extra_log_forget, head_norm_scale, mixer_output_matrix)
    expert_out = expert_part(expert_input_tokens, expert_norm_scale, routes, router_scores_chosen, expert_gate_matrix, expert_up_matrix, expert_down_matrix)
    return (mixer_output_rows, expert_out)
```

```python
import functools

import jax
import jax.numpy as jnp
from jax import lax
from jax.experimental import pallas as pl
from jax.experimental.pallas import tpu as pltpu
from jax.sharding import PartitionSpec as P

HEAD_DIM = 128
CHUNK = 64
MESH = pl.DeviceIdType.MESH
F32 = jnp.float32
BF16 = jnp.bfloat16


def flip(i, k):
    b = 1
    while b <= k:
        if k & b:
            i = i + b - 2 * b * lax.rem(lax.div(i, b), 2)
        b *= 2
    return i


def kernel(
    E, T, cap, near, groups, plan,
    q_hbm, f_hbm, v_hbm, o_hbm, gap_ref, extra_hbm, hscale_ref,
    mixw_hbm, tok_ref, escale_ref, routes_ref, scores_ref,
    gate_hbm, up_hbm, down_hbm,
    mix_out, exp_out,
    q_ref, f_ref, v_ref, o_ref, extra_ref,
    gate, up, down, mixw,
    ncols, dmat, wmat, outgoing, nearout, feats, hidden, part, precv, xsend, xrecv, fin, ret,
    qs, ks, run, qg, rec, ist, idec, est, bst, bdec, psum, pdec, ksend, krecv, csend, crecv,
    mhid, mpart, mprecv, mxsend, mxrecv,
    wsem, send_sem, recv_sem,
):
    me = lax.axis_index("ep")
    t = lax.axis_index("tp")
    G = T // 2
    g, c = lax.div(t, 2), lax.rem(t, 2)
    oc = 1 - c
    tokens, width = q_ref.shape
    heads = width // HEAD_DIM
    Dl = outgoing.shape[1]
    FFl = hidden.shape[1]

    loads = [
        pltpu.make_async_copy(src, dst, wsem.at[i])
        for i, (src, dst) in enumerate(
            (
                (f_hbm, f_ref), (extra_hbm, extra_ref), (q_hbm, q_ref), (v_hbm, v_ref),
                (gate_hbm, gate), (up_hbm, up), (down_hbm, down),
                (o_hbm, o_ref), (mixw_hbm, mixw),
            )
        )
    ]

    barrier = pltpu.get_barrier_semaphore()
    for k in range(1, E):
        pl.semaphore_signal(barrier, inc=1, device_id=(flip(me, k), t), device_id_type=MESH)
    pl.semaphore_signal(barrier, inc=1, device_id=(me, 2 * g + oc), device_id_type=MESH)
    for j in range(1, G):
        pl.semaphore_signal(
            barrier, inc=1, device_id=(me, 2 * flip(g, j) + c), device_id_type=MESH
        )

    for load in loads:
        load.start()

    used = [0]

    def remote(src, dst, device):
        slot = used[0]
        used[0] += 1
        return pltpu.make_async_remote_copy(
            src_ref=src, dst_ref=dst, send_sem=send_sem.at[slot], recv_sem=recv_sem.at[slot],
            device_id=device, device_id_type=MESH,
        )

    sent = []

    def launch(copy):
        copy.start()
        sent.append(copy)
        return copy

    x = tok_ref[...].astype(F32)
    mean = jnp.mean(x, axis=-1, keepdims=True)
    centred = x - mean
    inv = lax.rsqrt(jnp.mean(centred * centred, axis=-1, keepdims=True) + 1e-05)

    def normed(cols):
        return ((tok_ref[:, cols].astype(F32) - mean) * inv * escale_ref[:, cols]).astype(BF16)

    ntok = tok_ref.shape[0]
    ek = lax.broadcasted_iota(jnp.int32, (E, ntok), 0) ^ me
    first, second = routes_ref[0:1, :] == ek, routes_ref[1:2, :] == ek
    named = jnp.where(first | second, 1.0, 0.0)
    earlier = jnp.where(
        lax.broadcasted_iota(jnp.int32, (ntok, ntok), 0)
        < lax.broadcasted_iota(jnp.int32, (ntok, ntok), 1), 1.0, 0.0
    ).astype(BF16)
    position = jnp.dot(named.astype(BF16), earlier, preferred_element_type=F32)
    place = jnp.where(first | second, position, -1.0).astype(jnp.int32)
    rows = lax.broadcasted_iota(jnp.int32, (cap, ntok), 0)

    def choose(k):
        dmat[k * cap:(k + 1) * cap, :] = jnp.where(rows == place[k:k + 1, :], 1.0, 0.0).astype(BF16)

    for k in range(near, E):
        choose(k)
    own = normed(pl.ds(pl.multiple_of(t * Dl, 128), Dl))
    outgoing[...] = jnp.dot(
        dmat[near * cap:, :], own, preferred_element_type=F32
    ).astype(BF16)

    dispatch = {}
    order = [k for p in plan["far"] for k in range(groups[p][0], sum(groups[p]))]
    for k in order:
        dispatch[k] = remote(
            outgoing.at[pl.ds((k - near) * cap, cap)],
            feats.at[c, g, pl.ds(k * cap, cap)], (flip(me, k), t),
        )

    pl.semaphore_wait(barrier, E - 1 + 1 + G - 1)

    for k in order:
        launch(dispatch[k])

    for load in loads[:4]:
        load.wait()
    closing = gap_ref[...] * jax.nn.sigmoid(-f_ref[...].astype(F32))
    ks[...] = closing
    logd = jnp.log1p(-closing) + extra_ref[...]
    qs[...] = jax.nn.silu(q_ref[...].astype(F32))
    r_i = lax.broadcasted_iota(jnp.int32, (CHUNK, CHUNK), 0)
    c_i = lax.broadcasted_iota(jnp.int32, (CHUNK, CHUNK), 1)
    causal = r_i >= c_i
    tri = jnp.where(causal, 1.0, 0.0).astype(F32)
    nchunks = tokens // CHUNK
    for n in range(nchunks):
        run[n * CHUNK:(n + 1) * CHUNK, :] = jnp.dot(
            tri, logd[n * CHUNK:(n + 1) * CHUNK, :], precision=lax.Precision.HIGHEST,
            preferred_element_type=F32,
        )

    def head_local(h, _):
        lanes = pl.ds(pl.multiple_of(h * HEAD_DIM, HEAD_DIM), HEAD_DIM)
        state = jnp.zeros((HEAD_DIM, HEAD_DIM), F32)
        before = jnp.zeros((1, HEAD_DIM), F32)
        for n in range(nchunks):
            rs = slice(n * CHUNK, (n + 1) * CHUNK)
            r = run[rs, lanes]
            total = r[CHUNK - 1:CHUNK, :]
            qd = qs[rs, lanes] * jnp.exp(r)
            key = ks[rs, lanes]
            kd = (key * jnp.exp(-r)).astype(BF16)
            kst = (key * jnp.exp(total - r)).astype(BF16)
            val = v_ref[rs, lanes]
            qd_b = qd.astype(BF16)
            scores = lax.dot_general(
                qd_b, kd, (((1,), (1,)), ((), ())), preferred_element_type=F32
            )
            scores = jnp.where(causal, scores, 0.0).astype(BF16)
            out = jnp.dot(scores, val, preferred_element_type=F32)
            if n:
                out += lax.dot_general(
                    qd_b, state.astype(BF16), (((1,), (1,)), ((), ())),
                    preferred_element_type=F32,
                )
            rec[rs, lanes] = out
            qg[rs, lanes] = (qd * jnp.exp(before)).astype(BF16)
            state = state * jnp.exp(total) + lax.dot_general(
                val, kst, (((0,), (0,)), ((), ())), preferred_element_type=F32
            )
            before = before + total
        ist[h] = state
        idec[h] = jnp.broadcast_to(jnp.exp(before), (16, HEAD_DIM))
        return 0

    lax.fori_loop(0, heads, head_local, 0)

    odd = lax.rem(me, 2) == 1
    z = lax.div(me, 2)
    Z = E // 2
    ksend[:, 0:HEAD_DIM, :] = ist[...].astype(BF16)
    ksend[:, HEAD_DIM:, :] = idec[...].astype(BF16)
    pair = launch(remote(ksend, krecv, (flip(me, 1), t)))
    chain = remote(csend, crecv, (lax.rem(me + 2, E), t)) if Z > 1 else None

    def pair_end():
        pair.wait_recv()
        s = krecv[:, 0:HEAD_DIM, :].astype(F32)
        d = krecv[:, HEAD_DIM:, :].astype(F32)
        bst[...] = jnp.where(odd, s, 0.0)
        bdec[...] = jnp.where(odd, d, 1.0)
        psum[...] = jnp.where(
            odd, idec[:, 0:1, :] * s + ist[...], d[:, 0:1, :] * ist[...] + s
        )
        pdec[...] = idec[...] * d

    def chain_step(i):
        @pl.when(z == i)
        def _():
            if i:
                chain.wait_recv()
                carry = crecv[...].astype(F32)
                est[...] = bdec[:, 0:1, :] * carry + bst[...]
                if i + 1 < Z:
                    csend[...] = (pdec[:, 0:1, :] * carry + psum[...]).astype(BF16)
            else:
                est[...] = bst[...]
                if i + 1 < Z:
                    csend[...] = psum[...].astype(BF16)
            if i + 1 < Z:
                chain.start()

    for k in range(near):
        choose(k)
    for d in range(T):
        ncols[d % 2, d // 2] = normed(slice(d * Dl, (d + 1) * Dl))
    for j in range(G):
        nearout[j] = jnp.dot(
            dmat[cap:near * cap, :], ncols[c, j], preferred_element_type=F32
        ).astype(BF16)
    for k in range(1, near):
        dispatch[k] = launch(remote(
            nearout.at[:, pl.ds((k - 1) * cap, cap)],
            feats.at[c, :, pl.ds(k * cap, cap)], (flip(me, k), t),
        ))
    for d in range(T):
        feats[d % 2, d // 2, 0:cap, :] = jnp.dot(
            dmat[0:cap, :], ncols[d % 2, d // 2], preferred_element_type=F32
        ).astype(BF16)
    w0 = jax.nn.sigmoid(scores_ref[0:1, :] - scores_ref[1:2, :])
    weight = jnp.where(first, w0, jnp.where(second, 1.0 - w0, 0.0))
    for k in range(E):
        wmat[k * cap:(k + 1) * cap, :] = jnp.where(
            rows == place[k:k + 1, :], weight[k:k + 1, :], 0.0
        ).astype(BF16)

    ag_partner, ag_cross, rs_partner, rs_cross, back = {}, {}, {}, {}, {}
    partner = (me, 2 * g + oc)

    def piece_rows(p):
        a, n = groups[p]
        return pl.ds(a * cap, n * cap)

    def gather_start(p):
        a, n = groups[p]
        lo = max(a, 1)
        if lo == a + n:
            return
        for k in range(lo, a + n):
            dispatch[k].wait_recv()
        if a < near:
            rr = pl.ds(lo * cap, (a + n - lo) * cap)
            ag_partner[p, 0] = launch(remote(feats.at[c, :, rr], feats.at[c, :, rr], partner))
            return
        rr = piece_rows(p)
        for j in range(1, G):
            ag_cross[p, j] = launch(
                remote(feats.at[c, g, rr], feats.at[c, g, rr], (me, 2 * flip(g, j) + c))
            )
        ag_partner[p, 0] = launch(remote(feats.at[c, g, rr], feats.at[c, g, rr], partner))

    def gather_relay(p):
        rr = piece_rows(p)
        for j in range(1, G):
            ag_cross[p, j].wait_recv()
            gj = flip(g, j)
            ag_partner[p, j] = launch(remote(feats.at[c, gj, rr], feats.at[c, gj, rr], partner))

    def gather_end(p):
        for j in range(G):
            if (p, j) in ag_partner:
                ag_partner[p, j].wait_recv()

    tile = min(256, FFl)

    def experts(p):
        gather_end(p)
        a, n = groups[p]
        rs = slice(a * cap, (a + n) * cap)

        def one(i, _):
            cc = pl.ds(pl.multiple_of(i * tile, tile), tile)
            ga = jnp.zeros((n * cap, tile), F32)
            ua = jnp.zeros((n * cap, tile), F32)
            for d in range(T):
                xs = feats[d % 2, d // 2, rs, :]
                ga += jnp.dot(xs, gate[d * Dl:(d + 1) * Dl, cc], preferred_element_type=F32)
                ua += jnp.dot(xs, up[d * Dl:(d + 1) * Dl, cc], preferred_element_type=F32)
            hidden[rs, cc] = (jax.nn.silu(ga) * ua).astype(BF16)
            return 0

        lax.fori_loop(0, FFl // tile, one, 0)

        def down_group(cls, gg):
            ff = pl.ds(pl.multiple_of((2 * gg + cls) * Dl, 128), Dl)
            part[cls, gg, rs, :] = lax.dot_general(
                hidden[rs, :], down[ff, :], (((1,), (1,)), ((), ())),
                preferred_element_type=F32,
            ).astype(BF16)

        def theirs(gg, _):
            down_group(oc, gg)
            return 0

        def ours(gg, _):
            down_group(c, gg)
            return 0

        lax.fori_loop(0, G, theirs, 0)
        rr = piece_rows(p)
        rs_partner[p] = launch(remote(part.at[oc, :, rr], precv.at[:, rr], partner))
        lax.fori_loop(0, G, ours, 0)

    def scatter_cross(p):
        a, n = groups[p]
        rs = slice(a * cap, (a + n) * cap)
        rr = piece_rows(p)
        rs_partner[p].wait_recv()
        for j in range(1, G):
            gj = flip(g, j)
            xsend[j - 1, rs, :] = (
                part[c, gj, rs, :].astype(F32) + precv[gj, rs, :].astype(F32)
            ).astype(BF16)
            rs_cross[p, j] = launch(
                remote(xsend.at[j - 1, rr], xrecv.at[j - 1, rr], (me, 2 * gj + c))
            )

    def give_back(p):
        a, n = groups[p]
        rs = slice(a * cap, (a + n) * cap)
        total = part[c, g, rs, :].astype(F32) + precv[g, rs, :].astype(F32)
        for j in range(1, G):
            rs_cross[p, j].wait_recv()
            total += xrecv[j - 1, rs, :].astype(F32)
        fin[rs, :] = total.astype(BF16)
        for k in range(max(a, 1), a + n):
            block = pl.ds(k * cap, cap)
            back[k] = launch(remote(fin.at[block], ret.at[block], (flip(me, k), t)))
        if a == 0:
            ret[0:cap, :] = fin[0:cap, :]

    def mixer_end():
        for load in loads[7:]:
            load.wait()
        for h in range(heads):
            lanes = slice(h * HEAD_DIM, (h + 1) * HEAD_DIM)
            r = rec[:, lanes] + lax.dot_general(
                qg[:, lanes], est[h].astype(BF16), (((1,), (1,)), ((), ())),
                preferred_element_type=F32,
            )
            r = r * lax.rsqrt(jnp.mean(r * r, axis=-1, keepdims=True) + 1e-06)
            mhid[:, lanes] = (
                r * hscale_ref[:, lanes] * jax.nn.silu(o_ref[:, lanes].astype(F32))
            ).astype(BF16)
        R = mix_out.shape[0]
        wide = mixw.shape[1]
        step = min(512, wide)

        def one(i, _):
            cc = pl.ds(pl.multiple_of(i * step, step), step)
            y = jnp.dot(mhid[...], mixw[:, cc], preferred_element_type=F32).astype(BF16)
            for d in range(T):
                mpart[d % 2, d // 2, :, cc] = y[d * R:(d + 1) * R, :]
            return 0

        lax.fori_loop(0, wide // step, one, 0)
        rs_partner["m"] = launch(remote(mpart.at[oc], mprecv, partner))

    def mixer_cross():
        rs_partner["m"].wait_recv()
        for j in range(1, G):
            gj = flip(g, j)
            mxsend[j - 1] = (mpart[c, gj].astype(F32) + mprecv[gj].astype(F32)).astype(BF16)
            rs_cross["m", j] = launch(
                remote(mxsend.at[j - 1], mxrecv.at[j - 1], (me, 2 * gj + c))
            )

    def mixer_out():
        total = mpart[c, g].astype(F32) + mprecv[g].astype(F32)
        for j in range(1, G):
            rs_cross["m", j].wait_recv()
            total += mxrecv[j - 1].astype(F32)
        mix_out[...] = total.astype(BF16)

    def chain_rest():
        for i in range(plan["chain"], Z):
            chain_step(i)

    steps = {
        "a": gather_start, "b": gather_relay, "c": experts, "d": scatter_cross, "e": give_back,
        "pair": pair_end, "chain": chain_step, "chains": chain_rest,
        "mc": mixer_end, "md": mixer_cross, "me": mixer_out,
    }
    for load in loads[4:7]:
        load.wait()
    for step in plan["steps"]:
        steps[step[0]](*step[1:])
    for k in range(1, E):
        back[k].wait_recv()
    exp_out[...] = lax.dot_general(
        wmat[...], ret[...], (((0,), (0,)), ((), ())), preferred_element_type=F32
    ).astype(BF16)
    for copy in sent:
        copy.wait_send()
    if chain is not None:
        @pl.when(me + 2 < E)
        def _():
            chain.wait_send()


def make_plan(count):
    n = list(range(count // 2))
    f = list(range(count // 2, count))[::-1]
    steps = [
        "c n0", "a f0", "d n0", "pair", "chain 0", "a n1", "b f0", "a f1", "c f0", "b f1",
        "chain 1", "d f0", "a f2", "c n1", "c f1", "e n0", "e f0", "b f2", "d f1", "a f3",
        "a n2", "d n1", "chain 2", "c n2", "c f2", "e f1", "e n1", "b f3", "d f2", "a n3",
        "d n2", "chains", "c n3", "c f3", "e f2", "e n2", "d f3", "d n3", "mc", "e f3", "md",
        "e n3", "me",
    ]
    parsed = []
    for s in steps:
        name, *rest = s.split()
        where = [(n if r[0] == "n" else f)[int(r[1])] if r[0] in "nf" else int(r) for r in rest]
        parsed.append((name, *where))
    return {"far": f, "steps": parsed, "chain": 3}


def body(E, T, q, f, v, o, gap, extra, hscale, mixw, tok, escale, routes, scores, gate, up, down):
    tokens, width = q.shape
    ntok, D = tok.shape
    heads = width // HEAD_DIM
    G = T // 2
    cap = -(-(3 * ntok // E) // 16) * 16
    S = E * cap
    Dl = D // T
    FFl = gate.shape[2]
    R = tokens // T
    near = E // 2
    each = E // 8
    groups = tuple((i * each, each) for i in range(8))
    copies = 2 * (E - 1) + 2 + len(groups) * (G - 1 + G + 1 + G - 1) + G
    vm = pl.BlockSpec(memory_space=pltpu.VMEM)
    anyspace = pl.BlockSpec(memory_space=pl.ANY)
    V = pltpu.VMEM
    scratch = [
        V(q.shape, BF16), V(q.shape, BF16), V(q.shape, BF16), V(q.shape, BF16), V(q.shape, F32),
        V((D, FFl), BF16), V((D, FFl), BF16), V((D, FFl), BF16), V(mixw.shape, BF16),
        V((2, G, ntok, Dl), BF16), V((S, ntok), BF16), V((S, ntok), BF16),
        V(((E - near) * cap, Dl), BF16), V((G, (near - 1) * cap, Dl), BF16),
        V((2, G, S, Dl), BF16), V((S, FFl), BF16), V((2, G, S, Dl), BF16), V((G, S, Dl), BF16),
        V((max(G - 1, 1), S, Dl), BF16), V((max(G - 1, 1), S, Dl), BF16),
        V((S, Dl), BF16), V((S, Dl), BF16),
        V((tokens, width), F32), V((tokens, width), F32), V((tokens, width), F32),
        V((tokens, width), BF16), V((tokens, width), F32),
        V((heads, HEAD_DIM, HEAD_DIM), F32), V((heads, 16, HEAD_DIM), F32),
        V((heads, HEAD_DIM, HEAD_DIM), F32),
        V((heads, HEAD_DIM, HEAD_DIM), F32), V((heads, 16, HEAD_DIM), F32),
        V((heads, HEAD_DIM, HEAD_DIM), F32), V((heads, 16, HEAD_DIM), F32),
        V((heads, HEAD_DIM + 16, HEAD_DIM), BF16), V((heads, HEAD_DIM + 16, HEAD_DIM), BF16),
        V((heads, HEAD_DIM, HEAD_DIM), BF16), V((heads, HEAD_DIM, HEAD_DIM), BF16),
        V((tokens, width), BF16), V((2, G, R, D), BF16), V((G, R, D), BF16),
        V((max(G - 1, 1), R, D), BF16), V((max(G - 1, 1), R, D), BF16),
        pltpu.SemaphoreType.DMA((9,)),
        pltpu.SemaphoreType.DMA((copies,)),
        pltpu.SemaphoreType.DMA((copies,)),
    ]
    return pl.pallas_call(
        functools.partial(kernel, E, T, cap, near, groups, make_plan(len(groups))),
        out_shape=(
            jax.ShapeDtypeStruct((R, D), BF16),
            jax.ShapeDtypeStruct((ntok, Dl), BF16),
        ),
        in_specs=(
            [anyspace] * 4 + [vm, anyspace, vm, anyspace] + [vm] * 4 + [anyspace] * 3
        ),
        out_specs=(vm, vm),
        scratch_shapes=scratch,
        compiler_params=pltpu.CompilerParams(
            collective_id=0, has_side_effects=True, vmem_limit_bytes=60 * 1024 * 1024
        ),
    )(
        q, f, v, o, gap[None], extra, hscale[None], mixw, tok, escale[None],
        routes.T, scores.T, gate[0], up[0], down[0],
    )


def solution(mesh):
    E, T = mesh.shape["ep"], mesh.shape["tp"]
    return jax.shard_map(
        functools.partial(body, E, T),
        mesh=mesh,
        in_specs=(
            P("ep", "tp"),
            P("ep", "tp"),
            P("ep", "tp"),
            P("ep", "tp"),
            P("tp"),
            P("ep", "tp"),
            P("tp"),
            P("tp", None),
            P("ep", None),
            P(),
            P("ep", None),
            P("ep", None),
            P("ep", None, "tp"),
            P("ep", None, "tp"),
            P("ep", None, "tp"),
        ),
        out_specs=(P(("ep", "tp"), None), P("ep", "tp")),
        check_vma=False,
    )
```

```python
import functools

import jax
import jax.numpy as jnp
from jax import lax
from jax.experimental import pallas as pl
from jax.experimental.pallas import tpu as pltpu
from jax.sharding import PartitionSpec as P

HEAD_DIM = 128
CHUNK = 64
MESH = pl.DeviceIdType.MESH
F32 = jnp.float32
BF16 = jnp.bfloat16


def flip(i, k):
    b = 1
    while b <= k:
        if k & b:
            i = i + b - 2 * b * lax.rem(lax.div(i, b), 2)
        b *= 2
    return i


def kernel(
    E, T, cap, near, slots, each, plan,
    q_hbm, f_hbm, v_hbm, o_hbm, gap_ref, extra_hbm, hscale_ref,
    mixw_hbm, tok_ref, escale_ref, routes_ref, scores_ref,
    gate_hbm, up_hbm, down_hbm,
    mix_out, exp_out,
    q_ref, f_ref, v_ref, o_ref, extra_ref,
    gate, up, down, mixw,
    ncols, dmat, wmat, outgoing, nearout, feats, hidden, part, precv, xsend, xrecv, fin, ret,
    qs, ks, run, qg, rec, ist, idec, est, bst, bdec, psum, pdec, ksend, krecv, csend, crecv,
    mhid, mpart, mprecv, mxsend, mxrecv,
    wsem, send_sem, recv_sem,
):
    me = lax.axis_index("ep")
    t = lax.axis_index("tp")
    G = T // 2
    g, c = lax.div(t, 2), lax.rem(t, 2)
    oc = 1 - c
    tokens, width = q_ref.shape
    heads = width // HEAD_DIM
    Dl = outgoing.shape[1]
    FFl = hidden.shape[1]

    loads = [
        pltpu.make_async_copy(src, dst, wsem.at[i])
        for i, (src, dst) in enumerate(
            (
                (f_hbm, f_ref), (extra_hbm, extra_ref), (q_hbm, q_ref), (v_hbm, v_ref),
                (gate_hbm, gate), (up_hbm, up), (down_hbm, down),
                (o_hbm, o_ref), (mixw_hbm, mixw),
            )
        )
    ]

    barrier = pltpu.get_barrier_semaphore()
    for k in range(1, E):
        pl.semaphore_signal(barrier, inc=1, device_id=(flip(me, k), t), device_id_type=MESH)
    pl.semaphore_signal(barrier, inc=1, device_id=(me, 2 * g + oc), device_id_type=MESH)
    for j in range(1, G):
        pl.semaphore_signal(
            barrier, inc=1, device_id=(me, 2 * flip(g, j) + c), device_id_type=MESH
        )

    for load in loads:
        load.start()

    used = [0]

    def remote(src, dst, device):
        slot = used[0]
        used[0] += 1
        return pltpu.make_async_remote_copy(
            src_ref=src, dst_ref=dst, send_sem=send_sem.at[slot], recv_sem=recv_sem.at[slot],
            device_id=device, device_id_type=MESH,
        )

    sent = []

    def launch(copy):
        copy.start()
        sent.append(copy)
        return copy

    x = tok_ref[...].astype(F32)
    mean = jnp.mean(x, axis=-1, keepdims=True)
    centred = x - mean
    inv = lax.rsqrt(jnp.mean(centred * centred, axis=-1, keepdims=True) + 1e-05)

    def normed(cols):
        return ((tok_ref[:, cols].astype(F32) - mean) * inv * escale_ref[:, cols]).astype(BF16)

    ntok = tok_ref.shape[0]
    ek = lax.broadcasted_iota(jnp.int32, (E, ntok), 0) ^ me
    first, second = routes_ref[0:1, :] == ek, routes_ref[1:2, :] == ek
    named = jnp.where(first | second, 1.0, 0.0)
    earlier = jnp.where(
        lax.broadcasted_iota(jnp.int32, (ntok, ntok), 0)
        < lax.broadcasted_iota(jnp.int32, (ntok, ntok), 1), 1.0, 0.0
    ).astype(BF16)
    position = jnp.dot(named.astype(BF16), earlier, preferred_element_type=F32)
    place = jnp.where(first | second, position, -1.0).astype(jnp.int32)
    rows = lax.broadcasted_iota(jnp.int32, (cap, ntok), 0)

    def choose(i):
        k = slots[i]
        dmat[i * cap:(i + 1) * cap, :] = jnp.where(rows == place[k:k + 1, :], 1.0, 0.0).astype(BF16)

    for i in range(near, E):
        choose(i)
    own = normed(pl.ds(pl.multiple_of(t * Dl, 128), Dl))
    outgoing[...] = jnp.dot(
        dmat[near * cap:, :], own, preferred_element_type=F32
    ).astype(BF16)

    dispatch = {}

    def send_far(i):
        dispatch[i] = launch(remote(
            outgoing.at[pl.ds((i - near) * cap, cap)],
            feats.at[c, g, pl.ds(i * cap, cap)], (flip(me, slots[i]), t),
        ))

    def send_near(i):
        dispatch[i] = launch(remote(
            nearout.at[:, pl.ds((i - 1) * cap, cap)],
            feats.at[c, :, pl.ds(i * cap, cap)], (flip(me, slots[i]), t),
        ))

    pl.semaphore_wait(barrier, E - 1 + 1 + G - 1)

    def far_out(p):
        for i in range(p * each, (p + 1) * each):
            send_far(i)

    def near_out(p):
        for i in range(max(1, p * each), (p + 1) * each):
            send_near(i)

    def near_prepare():
        for i in range(near):
            choose(i)
        for d in range(T):
            ncols[d % 2, d // 2] = normed(slice(d * Dl, (d + 1) * Dl))
        for j in range(G):
            nearout[j] = jnp.dot(
                dmat[cap:near * cap, :], ncols[c, j], preferred_element_type=F32
            ).astype(BF16)

    def local_features():
        for d in range(T):
            feats[d % 2, d // 2, 0:cap, :] = jnp.dot(
                dmat[0:cap, :], ncols[d % 2, d // 2], preferred_element_type=F32
            ).astype(BF16)

    r_i = lax.broadcasted_iota(jnp.int32, (CHUNK, CHUNK), 0)
    c_i = lax.broadcasted_iota(jnp.int32, (CHUNK, CHUNK), 1)
    causal = r_i >= c_i
    nchunks = tokens // CHUNK

    def head_local(h, _):
        lanes = pl.ds(pl.multiple_of(h * HEAD_DIM, HEAD_DIM), HEAD_DIM)
        state = jnp.zeros((HEAD_DIM, HEAD_DIM), F32)
        before = jnp.zeros((1, HEAD_DIM), F32)
        for n in range(nchunks):
            rs = slice(n * CHUNK, (n + 1) * CHUNK)
            r = run[rs, lanes]
            total = r[CHUNK - 1:CHUNK, :]
            qd = qs[rs, lanes] * jnp.exp(r)
            key = ks[rs, lanes]
            kd = (key * jnp.exp(-r)).astype(BF16)
            kst = (key * jnp.exp(total - r)).astype(BF16)
            val = v_ref[rs, lanes]
            qd_b = qd.astype(BF16)
            scores = lax.dot_general(
                qd_b, kd, (((1,), (1,)), ((), ())), preferred_element_type=F32
            )
            scores = jnp.where(causal, scores, 0.0).astype(BF16)
            out = jnp.dot(scores, val, preferred_element_type=F32)
            if n:
                out += lax.dot_general(
                    qd_b, state.astype(BF16), (((1,), (1,)), ((), ())),
                    preferred_element_type=F32,
                )
            rec[rs, lanes] = out
            qg[rs, lanes] = (qd * jnp.exp(before)).astype(BF16)
            state = state * jnp.exp(total) + lax.dot_general(
                val, kst, (((0,), (0,)), ((), ())), preferred_element_type=F32
            )
            before = before + total
        ist[h] = state
        idec[h] = jnp.broadcast_to(jnp.exp(before), (16, HEAD_DIM))
        return 0

    odd = lax.rem(me, 2) == 1
    z = lax.div(me, 2)
    Z = E // 2
    pair = remote(ksend, krecv, (flip(me, 1), t))
    chain = remote(csend, crecv, (lax.rem(me + 2, E), t)) if Z > 1 else None

    def recurrence():
        for load in loads[:4]:
            load.wait()
        closing = gap_ref[...] * jax.nn.sigmoid(-f_ref[...].astype(F32))
        ks[...] = closing
        logd = jnp.log1p(-closing) + extra_ref[...]
        qs[...] = jax.nn.silu(q_ref[...].astype(F32))
        tri = jnp.where(causal, 1.0, 0.0).astype(F32)
        for n in range(nchunks):
            run[n * CHUNK:(n + 1) * CHUNK, :] = jnp.dot(
                tri, logd[n * CHUNK:(n + 1) * CHUNK, :], precision=lax.Precision.HIGHEST,
                preferred_element_type=F32,
            )

        lax.fori_loop(0, heads, head_local, 0)
        ksend[:, 0:HEAD_DIM, :] = ist[...].astype(BF16)
        ksend[:, HEAD_DIM:, :] = idec[...].astype(BF16)
        launch(pair)

    def pair_end():
        pair.wait_recv()
        s = krecv[:, 0:HEAD_DIM, :].astype(F32)
        d = krecv[:, HEAD_DIM:, :].astype(F32)
        bst[...] = jnp.where(odd, s, 0.0)
        bdec[...] = jnp.where(odd, d, 1.0)
        psum[...] = jnp.where(
            odd, idec[:, 0:1, :] * s + ist[...], d[:, 0:1, :] * ist[...] + s
        )
        pdec[...] = idec[...] * d

    def chain_step(i):
        @pl.when(z == i)
        def _():
            if i:
                chain.wait_recv()
                carry = crecv[...].astype(F32)
                est[...] = bdec[:, 0:1, :] * carry + bst[...]
                if i + 1 < Z:
                    csend[...] = (pdec[:, 0:1, :] * carry + psum[...]).astype(BF16)
            else:
                est[...] = bst[...]
                if i + 1 < Z:
                    csend[...] = psum[...].astype(BF16)
            if i + 1 < Z:
                chain.start()

    def weigh():
        w0 = jax.nn.sigmoid(scores_ref[0:1, :] - scores_ref[1:2, :])
        weight = jnp.where(first, w0, jnp.where(second, 1.0 - w0, 0.0))
        for i in range(E):
            k = slots[i]
            wmat[i * cap:(i + 1) * cap, :] = jnp.where(
                rows == place[k:k + 1, :], weight[k:k + 1, :], 0.0
            ).astype(BF16)

    ag_partner, ag_cross, rs_partner, rs_cross, back = {}, {}, {}, {}, {}
    partner = (me, 2 * g + oc)

    def unit(p):
        return p * each, each

    def piece_rows(p):
        return pl.ds(p * each * cap, each * cap)

    def gather_start(p):
        a, n = unit(p)
        lo = max(a, 1)
        if lo == a + n:
            return
        for i in range(lo, a + n):
            dispatch[i].wait_recv()
        if a < near:
            rr = pl.ds(lo * cap, (a + n - lo) * cap)
            ag_partner[p, 0] = launch(remote(feats.at[c, :, rr], feats.at[c, :, rr], partner))
            return
        rr = piece_rows(p)
        for j in range(1, G):
            ag_cross[p, j] = launch(
                remote(feats.at[c, g, rr], feats.at[c, g, rr], (me, 2 * flip(g, j) + c))
            )
        ag_partner[p, 0] = launch(remote(feats.at[c, g, rr], feats.at[c, g, rr], partner))

    def gather_relay(p):
        rr = piece_rows(p)
        for j in range(1, G):
            ag_cross[p, j].wait_recv()
            gj = flip(g, j)
            ag_partner[p, j] = launch(remote(feats.at[c, gj, rr], feats.at[c, gj, rr], partner))

    def gather_end(p):
        for j in range(G):
            if (p, j) in ag_partner:
                ag_partner[p, j].wait_recv()

    tile = min(256, FFl)

    def experts(*units):
        if not rs_partner:
            for load in loads[4:7]:
                load.wait()
        for p in units:
            gather_end(p)
        n = len(units) * each
        rs = slice(units[0] * each * cap, (units[-1] + 1) * each * cap)
        for i in range(FFl // tile):
            cc = slice(i * tile, (i + 1) * tile)
            ga = jnp.zeros((n * cap, tile), F32)
            ua = jnp.zeros((n * cap, tile), F32)
            for d in range(T):
                xs = feats[d % 2, d // 2, rs, :]
                ga += jnp.dot(xs, gate[d * Dl:(d + 1) * Dl, cc], preferred_element_type=F32)
                ua += jnp.dot(xs, up[d * Dl:(d + 1) * Dl, cc], preferred_element_type=F32)
            hidden[rs, cc] = (jax.nn.silu(ga) * ua).astype(BF16)

        def down_group(cls, gg):
            ff = pl.ds(pl.multiple_of((2 * gg + cls) * Dl, 128), Dl)
            part[cls, gg, rs, :] = lax.dot_general(
                hidden[rs, :], down[ff, :], (((1,), (1,)), ((), ())),
                preferred_element_type=F32,
            ).astype(BF16)

        for gg in range(G):
            down_group(oc, gg)
        for p in units:
            rr = piece_rows(p)
            rs_partner[p] = launch(remote(part.at[oc, :, rr], precv.at[:, rr], partner))
        for gg in range(G):
            down_group(c, gg)

    def scatter_cross(p):
        a, n = unit(p)
        rs = slice(a * cap, (a + n) * cap)
        rr = piece_rows(p)
        rs_partner[p].wait_recv()
        for j in range(1, G):
            gj = flip(g, j)
            xsend[j - 1, rs, :] = (
                part[c, gj, rs, :].astype(F32) + precv[gj, rs, :].astype(F32)
            ).astype(BF16)
            rs_cross[p, j] = launch(
                remote(xsend.at[j - 1, rr], xrecv.at[j - 1, rr], (me, 2 * gj + c))
            )

    def give_back(p):
        a, n = unit(p)
        rs = slice(a * cap, (a + n) * cap)
        total = part[c, g, rs, :].astype(F32) + precv[g, rs, :].astype(F32)
        for j in range(1, G):
            rs_cross[p, j].wait_recv()
            total += xrecv[j - 1, rs, :].astype(F32)
        fin[rs, :] = total.astype(BF16)
        for i in range(max(a, 1), a + n):
            block = pl.ds(i * cap, cap)
            back[i] = launch(remote(fin.at[block], ret.at[block], (flip(me, slots[i]), t)))
        if a == 0:
            ret[0:cap, :] = fin[0:cap, :]

    def mixer_end():
        for load in loads[7:]:
            load.wait()
        for h in range(heads):
            lanes = slice(h * HEAD_DIM, (h + 1) * HEAD_DIM)
            r = rec[:, lanes] + lax.dot_general(
                qg[:, lanes], est[h].astype(BF16), (((1,), (1,)), ((), ())),
                preferred_element_type=F32,
            )
            r = r * lax.rsqrt(jnp.mean(r * r, axis=-1, keepdims=True) + 1e-06)
            mhid[:, lanes] = (
                r * hscale_ref[:, lanes] * jax.nn.silu(o_ref[:, lanes].astype(F32))
            ).astype(BF16)
        R = mix_out.shape[0]
        wide = mixw.shape[1]
        step = min(512, wide)

        def one(i, _):
            cc = pl.ds(pl.multiple_of(i * step, step), step)
            y = jnp.dot(mhid[...], mixw[:, cc], preferred_element_type=F32).astype(BF16)
            for d in range(T):
                mpart[d % 2, d // 2, :, cc] = y[d * R:(d + 1) * R, :]
            return 0

        lax.fori_loop(0, wide // step, one, 0)
        rs_partner["m"] = launch(remote(mpart.at[oc], mprecv, partner))

    def mixer_cross():
        rs_partner["m"].wait_recv()
        for j in range(1, G):
            gj = flip(g, j)
            mxsend[j - 1] = (mpart[c, gj].astype(F32) + mprecv[gj].astype(F32)).astype(BF16)
            rs_cross["m", j] = launch(
                remote(mxsend.at[j - 1], mxrecv.at[j - 1], (me, 2 * gj + c))
            )

    def mixer_out():
        total = mpart[c, g].astype(F32) + mprecv[g].astype(F32)
        for j in range(1, G):
            rs_cross["m", j].wait_recv()
            total += mxrecv[j - 1].astype(F32)
        mix_out[...] = total.astype(BF16)

    def chain_rest(i):
        for i in range(i, Z):
            chain_step(i)

    steps = {
        "f": far_out, "n": near_out, "p": near_prepare, "l": local_features, "h": recurrence,
        "a": gather_start, "b": gather_relay, "c": experts, "d": scatter_cross, "e": give_back,
        "pair": pair_end, "chain": chain_step, "chains": chain_rest,
        "w": weigh, "mc": mixer_end, "md": mixer_cross, "me": mixer_out,
    }
    for step in plan:
        steps[step[0]](*step[1:])
    for k in range(1, E):
        back[k].wait_recv()
    exp_out[...] = lax.dot_general(
        wmat[...], ret[...], (((0,), (0,)), ((), ())), preferred_element_type=F32
    ).astype(BF16)
    for copy in sent:
        copy.wait_send()
    if chain is not None:
        @pl.when(me + 2 < E)
        def _():
            chain.wait_send()


STEPS = (
    "f 4", "f 5", "p", "n 1", "h", "f 6", "f 7", "n 2", "l", "c 0", "a 1", "a 4",
    "d 0", "n 3", "c 1", "a 5", "b 4", "a 6", "d 1",
    "c 4", "b 5", "d 4", "a 7", "pair", "chain 0", "c 5", "b 6", "e 0", "d 5", "a 2", "e 1",
    "c 6", "b 7", "e 4", "a 3", "d 6", "chain 1", "c 7",
    "e 5", "d 7", "c 2 3", "chain 2", "e 6", "d 2", "d 3", "chains 3", "mc", "e 7", "md", "w",
    "e 2", "e 3", "me",
)


def make_plan():
    return [(s[0], *(int(i) for i in s[1:])) for s in map(str.split, STEPS)]


def body(E, T, q, f, v, o, gap, extra, hscale, mixw, tok, escale, routes, scores, gate, up, down):
    tokens, width = q.shape
    ntok, D = tok.shape
    heads = width // HEAD_DIM
    G = T // 2
    cap = -(-(3 * ntok // E) // 16) * 16
    S = E * cap
    Dl = D // T
    FFl = gate.shape[2]
    R = tokens // T
    near = E // 2
    each = E // 8
    far = list(range(near, E))[::-1]
    slots = list(range(near)) + far[1::2] + far[0::2]
    copies = 2 * (E - 1) + 2 + 8 * (G - 1 + G + 1 + G - 1) + G
    vm = pl.BlockSpec(memory_space=pltpu.VMEM)
    anyspace = pl.BlockSpec(memory_space=pl.ANY)
    V = pltpu.VMEM
    scratch = [
        V(q.shape, BF16), V(q.shape, BF16), V(q.shape, BF16), V(q.shape, BF16), V(q.shape, F32),
        V((D, FFl), BF16), V((D, FFl), BF16), V((D, FFl), BF16), V(mixw.shape, BF16),
        V((2, G, ntok, Dl), BF16), V((S, ntok), BF16), V((S, ntok), BF16),
        V(((E - near) * cap, Dl), BF16), V((G, (near - 1) * cap, Dl), BF16),
        V((2, G, S, Dl), BF16), V((S, FFl), BF16), V((2, G, S, Dl), BF16), V((G, S, Dl), BF16),
        V((max(G - 1, 1), S, Dl), BF16), V((max(G - 1, 1), S, Dl), BF16),
        V((S, Dl), BF16), V((S, Dl), BF16),
        V((tokens, width), F32), V((tokens, width), F32), V((tokens, width), F32),
        V((tokens, width), BF16), V((tokens, width), F32),
        V((heads, HEAD_DIM, HEAD_DIM), F32), V((heads, 16, HEAD_DIM), F32),
        V((heads, HEAD_DIM, HEAD_DIM), F32),
        V((heads, HEAD_DIM, HEAD_DIM), F32), V((heads, 16, HEAD_DIM), F32),
        V((heads, HEAD_DIM, HEAD_DIM), F32), V((heads, 16, HEAD_DIM), F32),
        V((heads, HEAD_DIM + 16, HEAD_DIM), BF16), V((heads, HEAD_DIM + 16, HEAD_DIM), BF16),
        V((heads, HEAD_DIM, HEAD_DIM), BF16), V((heads, HEAD_DIM, HEAD_DIM), BF16),
        V((tokens, width), BF16), V((2, G, R, D), BF16), V((G, R, D), BF16),
        V((max(G - 1, 1), R, D), BF16), V((max(G - 1, 1), R, D), BF16),
        pltpu.SemaphoreType.DMA((9,)),
        pltpu.SemaphoreType.DMA((copies,)),
        pltpu.SemaphoreType.DMA((copies,)),
    ]
    return pl.pallas_call(
        functools.partial(kernel, E, T, cap, near, slots, each, make_plan()),
        out_shape=(
            jax.ShapeDtypeStruct((R, D), BF16),
            jax.ShapeDtypeStruct((ntok, Dl), BF16),
        ),
        in_specs=(
            [anyspace] * 4 + [vm, anyspace, vm, anyspace] + [vm] * 4 + [anyspace] * 3
        ),
        out_specs=(vm, vm),
        scratch_shapes=scratch,
        compiler_params=pltpu.CompilerParams(
            collective_id=0, has_side_effects=True, vmem_limit_bytes=60 * 1024 * 1024
        ),
    )(
        q, f, v, o, gap[None], extra, hscale[None], mixw, tok, escale[None],
        routes.T, scores.T, gate[0], up[0], down[0],
    )


def solution(mesh):
    E, T = mesh.shape["ep"], mesh.shape["tp"]
    return jax.shard_map(
        functools.partial(body, E, T),
        mesh=mesh,
        in_specs=(
            P("ep", "tp"),
            P("ep", "tp"),
            P("ep", "tp"),
            P("ep", "tp"),
            P("tp"),
            P("ep", "tp"),
            P("tp"),
            P("tp", None),
            P("ep", None),
            P(),
            P("ep", None),
            P("ep", None),
            P("ep", None, "tp"),
            P("ep", None, "tp"),
            P("ep", None, "tp"),
        ),
        out_specs=(P(("ep", "tp"), None), P("ep", "tp")),
        check_vma=False,
    )
```

```python
import functools

import jax
import jax.numpy as jnp
from jax import lax
from jax.experimental import pallas as pl
from jax.experimental.pallas import tpu as pltpu
from jax.sharding import PartitionSpec as P

HEAD_DIM = 128
CHUNK = 64
MESH = pl.DeviceIdType.MESH
F32 = jnp.float32
BF16 = jnp.bfloat16


def flip(i, k):
    b = 1
    while b <= k:
        if k & b:
            i = i + b - 2 * b * lax.rem(lax.div(i, b), 2)
        b *= 2
    return i


def kernel(
    E, T, cap, near, slots, each, plan,
    q_hbm, f_hbm, v_hbm, o_hbm, gap_ref, extra_hbm, hscale_ref,
    mixw_hbm, tok_ref, escale_ref, routes_ref, scores_ref,
    gate_hbm, up_hbm, down_hbm,
    mix_out, exp_out,
    q_ref, f_ref, v_ref, o_ref, extra_ref,
    gate, up, down, mixw,
    ncols, dmat, wmat, outgoing, nearout, feats, hidden, part, precv, xsend, xrecv, fin, ret,
    qs, ks, run, qg, rec, ist, idec, est, bst, bdec, psum, pdec, ksend, krecv, csend, crecv,
    mhid, mpart, mprecv, mxsend, mxrecv,
    wsem, send_sem, recv_sem,
):
    me = lax.axis_index("ep")
    t = lax.axis_index("tp")
    G = T // 2
    g, c = lax.div(t, 2), lax.rem(t, 2)
    oc = 1 - c
    tokens, width = q_ref.shape
    heads = width // HEAD_DIM
    Dl = outgoing.shape[1]
    FFl = hidden.shape[1]

    loads = [
        pltpu.make_async_copy(src, dst, wsem.at[i])
        for i, (src, dst) in enumerate(
            (
                (f_hbm, f_ref), (extra_hbm, extra_ref), (q_hbm, q_ref), (v_hbm, v_ref),
                (gate_hbm, gate), (up_hbm, up), (down_hbm, down),
                (o_hbm, o_ref), (mixw_hbm, mixw),
            )
        )
    ]

    barrier = pltpu.get_barrier_semaphore()
    for k in range(1, E):
        pl.semaphore_signal(barrier, inc=1, device_id=(flip(me, k), t), device_id_type=MESH)
    pl.semaphore_signal(barrier, inc=1, device_id=(me, 2 * g + oc), device_id_type=MESH)
    for j in range(1, G):
        pl.semaphore_signal(
            barrier, inc=1, device_id=(me, 2 * flip(g, j) + c), device_id_type=MESH
        )

    for load in loads:
        load.start()

    used = [0]

    def remote(src, dst, device):
        slot = used[0]
        used[0] += 1
        return pltpu.make_async_remote_copy(
            src_ref=src, dst_ref=dst, send_sem=send_sem.at[slot], recv_sem=recv_sem.at[slot],
            device_id=device, device_id_type=MESH,
        )

    sent = []

    def launch(copy):
        copy.start()
        sent.append(copy)
        return copy

    x = tok_ref[...].astype(F32)
    mean = jnp.mean(x, axis=-1, keepdims=True)
    centred = x - mean
    inv = lax.rsqrt(jnp.mean(centred * centred, axis=-1, keepdims=True) + 1e-05)

    def normed(cols):
        return ((tok_ref[:, cols].astype(F32) - mean) * inv * escale_ref[:, cols]).astype(BF16)

    ntok = tok_ref.shape[0]
    ek = lax.broadcasted_iota(jnp.int32, (E, ntok), 0) ^ me
    first, second = routes_ref[0:1, :] == ek, routes_ref[1:2, :] == ek
    named = jnp.where(first | second, 1.0, 0.0)
    earlier = jnp.where(
        lax.broadcasted_iota(jnp.int32, (ntok, ntok), 0)
        < lax.broadcasted_iota(jnp.int32, (ntok, ntok), 1), 1.0, 0.0
    ).astype(BF16)
    position = jnp.dot(named.astype(BF16), earlier, preferred_element_type=F32)
    place = jnp.where(first | second, position, -1.0).astype(jnp.int32)
    rows = lax.broadcasted_iota(jnp.int32, (cap, ntok), 0)

    def choose(i):
        k = slots[i]
        dmat[i * cap:(i + 1) * cap, :] = jnp.where(rows == place[k:k + 1, :], 1.0, 0.0).astype(BF16)

    for i in range(near, E):
        choose(i)
    own = normed(pl.ds(pl.multiple_of(t * Dl, 128), Dl))
    outgoing[...] = jnp.dot(
        dmat[near * cap:, :], own, preferred_element_type=F32
    ).astype(BF16)

    dispatch = {}

    def send_far(i):
        dispatch[i] = launch(remote(
            outgoing.at[pl.ds((i - near) * cap, cap)],
            feats.at[c, g, pl.ds(i * cap, cap)], (flip(me, slots[i]), t),
        ))

    def send_near(i):
        dispatch[i] = launch(remote(
            nearout.at[:, pl.ds((i - 1) * cap, cap)],
            feats.at[c, :, pl.ds(i * cap, cap)], (flip(me, slots[i]), t),
        ))

    pl.semaphore_wait(barrier, E - 1 + 1 + G - 1)

    def far_out(p):
        for i in range(p * each, (p + 1) * each):
            send_far(i)

    def near_out(p):
        for i in range(max(1, p * each), (p + 1) * each):
            send_near(i)

    def near_prepare():
        for i in range(near):
            choose(i)
        for d in range(T):
            ncols[d % 2, d // 2] = normed(slice(d * Dl, (d + 1) * Dl))
        for j in range(G):
            nearout[j] = jnp.dot(
                dmat[cap:near * cap, :], ncols[c, j], preferred_element_type=F32
            ).astype(BF16)

    def local_features():
        for d in range(T):
            feats[d % 2, d // 2, 0:cap, :] = jnp.dot(
                dmat[0:cap, :], ncols[d % 2, d // 2], preferred_element_type=F32
            ).astype(BF16)

    r_i = lax.broadcasted_iota(jnp.int32, (CHUNK, CHUNK), 0)
    c_i = lax.broadcasted_iota(jnp.int32, (CHUNK, CHUNK), 1)
    causal = r_i >= c_i
    nchunks = tokens // CHUNK

    def head_local(h, _):
        lanes = pl.ds(pl.multiple_of(h * HEAD_DIM, HEAD_DIM), HEAD_DIM)
        state = jnp.zeros((HEAD_DIM, HEAD_DIM), F32)
        before = jnp.zeros((1, HEAD_DIM), F32)
        for n in range(nchunks):
            rs = slice(n * CHUNK, (n + 1) * CHUNK)
            r = run[rs, lanes]
            total = r[CHUNK - 1:CHUNK, :]
            qd = qs[rs, lanes] * jnp.exp(r)
            key = ks[rs, lanes]
            kd = (key * jnp.exp(-r)).astype(BF16)
            kst = (key * jnp.exp(total - r)).astype(BF16)
            val = v_ref[rs, lanes]
            qd_b = qd.astype(BF16)
            scores = lax.dot_general(
                qd_b, kd, (((1,), (1,)), ((), ())), preferred_element_type=F32
            )
            scores = jnp.where(causal, scores, 0.0).astype(BF16)
            out = jnp.dot(scores, val, preferred_element_type=F32)
            if n:
                out += lax.dot_general(
                    qd_b, state.astype(BF16), (((1,), (1,)), ((), ())),
                    preferred_element_type=F32,
                )
            rec[rs, lanes] = out
            qg[rs, lanes] = (qd * jnp.exp(before)).astype(BF16)
            state = state * jnp.exp(total) + lax.dot_general(
                val, kst, (((0,), (0,)), ((), ())), preferred_element_type=F32
            )
            before = before + total
        ist[h] = state
        idec[h] = jnp.broadcast_to(jnp.exp(before), (16, HEAD_DIM))
        return 0

    odd = lax.rem(me, 2) == 1
    z = lax.div(me, 2)
    Z = E // 2
    pair = remote(ksend, krecv, (flip(me, 1), t))
    chain = remote(csend, crecv, (lax.rem(me + 2, E), t)) if Z > 1 else None

    def recurrence():
        for load in loads[:4]:
            load.wait()
        closing = gap_ref[...] * jax.nn.sigmoid(-f_ref[...].astype(F32))
        ks[...] = closing
        logd = jnp.log1p(-closing) + extra_ref[...]
        qs[...] = jax.nn.silu(q_ref[...].astype(F32))
        tri = jnp.where(causal, 1.0, 0.0).astype(F32)
        for n in range(nchunks):
            run[n * CHUNK:(n + 1) * CHUNK, :] = jnp.dot(
                tri, logd[n * CHUNK:(n + 1) * CHUNK, :], precision=lax.Precision.HIGHEST,
                preferred_element_type=F32,
            )

        lax.fori_loop(0, heads, head_local, 0)
        ksend[:, 0:HEAD_DIM, :] = ist[...].astype(BF16)
        ksend[:, HEAD_DIM:, :] = idec[...].astype(BF16)
        launch(pair)

    def pair_end():
        pair.wait_recv()
        s = krecv[:, 0:HEAD_DIM, :].astype(F32)
        d = krecv[:, HEAD_DIM:, :].astype(F32)
        bst[...] = jnp.where(odd, s, 0.0)
        bdec[...] = jnp.where(odd, d, 1.0)
        psum[...] = jnp.where(
            odd, idec[:, 0:1, :] * s + ist[...], d[:, 0:1, :] * ist[...] + s
        )
        pdec[...] = idec[...] * d

    def chain_step(i):
        @pl.when(z == i)
        def _():
            if i:
                chain.wait_recv()
                carry = crecv[...].astype(F32)
                est[...] = bdec[:, 0:1, :] * carry + bst[...]
                if i + 1 < Z:
                    csend[...] = (pdec[:, 0:1, :] * carry + psum[...]).astype(BF16)
            else:
                est[...] = bst[...]
                if i + 1 < Z:
                    csend[...] = psum[...].astype(BF16)
            if i + 1 < Z:
                chain.start()

    def weigh():
        w0 = jax.nn.sigmoid(scores_ref[0:1, :] - scores_ref[1:2, :])
        weight = jnp.where(first, w0, jnp.where(second, 1.0 - w0, 0.0))
        for i in range(E):
            k = slots[i]
            wmat[i * cap:(i + 1) * cap, :] = jnp.where(
                rows == place[k:k + 1, :], weight[k:k + 1, :], 0.0
            ).astype(BF16)

    ag_partner, ag_cross, rs_partner, rs_cross, back = {}, {}, {}, {}, {}
    partner = (me, 2 * g + oc)

    def unit(p):
        return p * each, each

    def piece_rows(p):
        return pl.ds(p * each * cap, each * cap)

    def gather_start(p):
        a, n = unit(p)
        lo = max(a, 1)
        if lo == a + n:
            return
        for i in range(lo, a + n):
            dispatch[i].wait_recv()
        if a < near:
            rr = pl.ds(lo * cap, (a + n - lo) * cap)
            ag_partner[p, 0] = launch(remote(feats.at[c, :, rr], feats.at[c, :, rr], partner))
            return
        rr = piece_rows(p)
        for j in range(1, G):
            ag_cross[p, j] = launch(
                remote(feats.at[c, g, rr], feats.at[c, g, rr], (me, 2 * flip(g, j) + c))
            )
        ag_partner[p, 0] = launch(remote(feats.at[c, g, rr], feats.at[c, g, rr], partner))

    def gather_relay(p):
        rr = piece_rows(p)
        for j in range(1, G):
            ag_cross[p, j].wait_recv()
            gj = flip(g, j)
            ag_partner[p, j] = launch(remote(feats.at[c, gj, rr], feats.at[c, gj, rr], partner))

    def gather_end(p):
        for j in range(G):
            if (p, j) in ag_partner:
                ag_partner[p, j].wait_recv()

    tile = min(256, FFl)

    def experts(*units):
        if not rs_partner:
            for load in loads[4:7]:
                load.wait()
        for p in units:
            gather_end(p)
        n = len(units) * each
        rs = slice(units[0] * each * cap, (units[-1] + 1) * each * cap)
        for i in range(FFl // tile):
            cc = slice(i * tile, (i + 1) * tile)
            ga = jnp.zeros((n * cap, tile), F32)
            ua = jnp.zeros((n * cap, tile), F32)
            for d in range(T):
                xs = feats[d % 2, d // 2, rs, :]
                ga += jnp.dot(xs, gate[d * Dl:(d + 1) * Dl, cc], preferred_element_type=F32)
                ua += jnp.dot(xs, up[d * Dl:(d + 1) * Dl, cc], preferred_element_type=F32)
            hidden[rs, cc] = (jax.nn.silu(ga) * ua).astype(BF16)

        def down_group(cls, gg):
            ff = pl.ds(pl.multiple_of((2 * gg + cls) * Dl, 128), Dl)
            part[cls, gg, rs, :] = lax.dot_general(
                hidden[rs, :], down[ff, :], (((1,), (1,)), ((), ())),
                preferred_element_type=F32,
            ).astype(BF16)

        for gg in range(G):
            down_group(oc, gg)
        for p in units:
            rr = piece_rows(p)
            rs_partner[p] = launch(remote(part.at[oc, :, rr], precv.at[:, rr], partner))
        for gg in range(G):
            down_group(c, gg)

    def scatter_cross(p):
        a, n = unit(p)
        rs = slice(a * cap, (a + n) * cap)
        rr = piece_rows(p)
        rs_partner[p].wait_recv()
        for j in range(1, G):
            gj = flip(g, j)
            xsend[j - 1, rs, :] = (
                part[c, gj, rs, :].astype(F32) + precv[gj, rs, :].astype(F32)
            ).astype(BF16)
            rs_cross[p, j] = launch(
                remote(xsend.at[j - 1, rr], xrecv.at[j - 1, rr], (me, 2 * gj + c))
            )

    def give_back(p):
        a, n = unit(p)
        rs = slice(a * cap, (a + n) * cap)
        total = part[c, g, rs, :].astype(F32) + precv[g, rs, :].astype(F32)
        for j in range(1, G):
            rs_cross[p, j].wait_recv()
            total += xrecv[j - 1, rs, :].astype(F32)
        fin[rs, :] = total.astype(BF16)
        for i in range(max(a, 1), a + n):
            block = pl.ds(i * cap, cap)
            back[i] = launch(remote(fin.at[block], ret.at[block], (flip(me, slots[i]), t)))
        if a == 0:
            ret[0:cap, :] = fin[0:cap, :]

    def mixer_end():
        for load in loads[7:]:
            load.wait()
        for h in range(heads):
            lanes = slice(h * HEAD_DIM, (h + 1) * HEAD_DIM)
            r = rec[:, lanes] + lax.dot_general(
                qg[:, lanes], est[h].astype(BF16), (((1,), (1,)), ((), ())),
                preferred_element_type=F32,
            )
            r = r * lax.rsqrt(jnp.mean(r * r, axis=-1, keepdims=True) + 1e-06)
            mhid[:, lanes] = (
                r * hscale_ref[:, lanes] * jax.nn.silu(o_ref[:, lanes].astype(F32))
            ).astype(BF16)
        R = mix_out.shape[0]
        wide = mixw.shape[1]
        step = min(512, wide)

        def one(i, _):
            cc = pl.ds(pl.multiple_of(i * step, step), step)
            y = jnp.dot(mhid[...], mixw[:, cc], preferred_element_type=F32).astype(BF16)
            for d in range(T):
                mpart[d % 2, d // 2, :, cc] = y[d * R:(d + 1) * R, :]
            return 0

        lax.fori_loop(0, wide // step, one, 0)
        rs_partner["m"] = launch(remote(mpart.at[oc], mprecv, partner))

    def mixer_cross():
        rs_partner["m"].wait_recv()
        for j in range(1, G):
            gj = flip(g, j)
            mxsend[j - 1] = (mpart[c, gj].astype(F32) + mprecv[gj].astype(F32)).astype(BF16)
            rs_cross["m", j] = launch(
                remote(mxsend.at[j - 1], mxrecv.at[j - 1], (me, 2 * gj + c))
            )

    def mixer_out():
        total = mpart[c, g].astype(F32) + mprecv[g].astype(F32)
        for j in range(1, G):
            rs_cross["m", j].wait_recv()
            total += mxrecv[j - 1].astype(F32)
        mix_out[...] = total.astype(BF16)

    def chain_rest(i):
        for i in range(i, Z):
            chain_step(i)

    steps = {
        "f": far_out, "n": near_out, "p": near_prepare, "l": local_features, "h": recurrence,
        "a": gather_start, "b": gather_relay, "c": experts, "d": scatter_cross, "e": give_back,
        "pair": pair_end, "chain": chain_step, "chains": chain_rest,
        "w": weigh, "mc": mixer_end, "md": mixer_cross, "me": mixer_out,
    }
    for step in plan:
        steps[step[0]](*step[1:])
    for k in range(1, E):
        back[k].wait_recv()
    exp_out[...] = lax.dot_general(
        wmat[...], ret[...], (((0,), (0,)), ((), ())), preferred_element_type=F32
    ).astype(BF16)
    for copy in sent:
        copy.wait_send()
    if chain is not None:
        @pl.when(me + 2 < E)
        def _():
            chain.wait_send()


STEPS = (
    "f 4", "f 5", "p", "n 1", "n 2", "h", "f 6", "f 7", "n 3", "l", "c 0", "a 1",
    "d 0", "c 1", "a 4", "a 2", "pair", "chain 0", "a 5", "d 1", "c 2", "b 4", "b 5", "a 6",
    "a 7",
    "c 4 5", "e 0", "chain 1", "e 1", "d 4", "d 5", "d 2", "a 3", "c 3", "b 6", "b 7", "chain 2",
    "e 4", "c 6 7", "e 5", "d 6", "d 7", "d 3", "e 2", "chains 3", "mc", "e 6", "md", "e 7",
    "w", "e 3", "me",
)


def make_plan():
    return [(s[0], *(int(i) for i in s[1:])) for s in map(str.split, STEPS)]


def body(E, T, q, f, v, o, gap, extra, hscale, mixw, tok, escale, routes, scores, gate, up, down):
    tokens, width = q.shape
    ntok, D = tok.shape
    heads = width // HEAD_DIM
    G = T // 2
    cap = -(-(3 * ntok // E) // 16) * 16
    S = E * cap
    Dl = D // T
    FFl = gate.shape[2]
    R = tokens // T
    near = E // 2
    each = E // 8
    far = list(range(near, E))[::-1]
    slots = list(range(near)) + far[1::2] + far[0::2]
    copies = 2 * (E - 1) + 2 + 8 * (G - 1 + G + 1 + G - 1) + G
    vm = pl.BlockSpec(memory_space=pltpu.VMEM)
    anyspace = pl.BlockSpec(memory_space=pl.ANY)
    V = pltpu.VMEM
    scratch = [
        V(q.shape, BF16), V(q.shape, BF16), V(q.shape, BF16), V(q.shape, BF16), V(q.shape, F32),
        V((D, FFl), BF16), V((D, FFl), BF16), V((D, FFl), BF16), V(mixw.shape, BF16),
        V((2, G, ntok, Dl), BF16), V((S, ntok), BF16), V((S, ntok), BF16),
        V(((E - near) * cap, Dl), BF16), V((G, (near - 1) * cap, Dl), BF16),
        V((2, G, S, Dl), BF16), V((S, FFl), BF16), V((2, G, S, Dl), BF16), V((G, S, Dl), BF16),
        V((max(G - 1, 1), S, Dl), BF16), V((max(G - 1, 1), S, Dl), BF16),
        V((S, Dl), BF16), V((S, Dl), BF16),
        V((tokens, width), F32), V((tokens, width), F32), V((tokens, width), F32),
        V((tokens, width), BF16), V((tokens, width), F32),
        V((heads, HEAD_DIM, HEAD_DIM), F32), V((heads, 16, HEAD_DIM), F32),
        V((heads, HEAD_DIM, HEAD_DIM), F32),
        V((heads, HEAD_DIM, HEAD_DIM), F32), V((heads, 16, HEAD_DIM), F32),
        V((heads, HEAD_DIM, HEAD_DIM), F32), V((heads, 16, HEAD_DIM), F32),
        V((heads, HEAD_DIM + 16, HEAD_DIM), BF16), V((heads, HEAD_DIM + 16, HEAD_DIM), BF16),
        V((heads, HEAD_DIM, HEAD_DIM), BF16), V((heads, HEAD_DIM, HEAD_DIM), BF16),
        V((tokens, width), BF16), V((2, G, R, D), BF16), V((G, R, D), BF16),
        V((max(G - 1, 1), R, D), BF16), V((max(G - 1, 1), R, D), BF16),
        pltpu.SemaphoreType.DMA((9,)),
        pltpu.SemaphoreType.DMA((copies,)),
        pltpu.SemaphoreType.DMA((copies,)),
    ]
    return pl.pallas_call(
        functools.partial(kernel, E, T, cap, near, slots, each, make_plan()),
        out_shape=(
            jax.ShapeDtypeStruct((R, D), BF16),
            jax.ShapeDtypeStruct((ntok, Dl), BF16),
        ),
        in_specs=(
            [anyspace] * 4 + [vm, anyspace, vm, anyspace] + [vm] * 4 + [anyspace] * 3
        ),
        out_specs=(vm, vm),
        scratch_shapes=scratch,
        compiler_params=pltpu.CompilerParams(
            collective_id=0, has_side_effects=True, vmem_limit_bytes=60 * 1024 * 1024
        ),
    )(
        q, f, v, o, gap[None], extra, hscale[None], mixw, tok, escale[None],
        routes.T, scores.T, gate[0], up[0], down[0],
    )


def solution(mesh):
    E, T = mesh.shape["ep"], mesh.shape["tp"]
    return jax.shard_map(
        functools.partial(body, E, T),
        mesh=mesh,
        in_specs=(
            P("ep", "tp"),
            P("ep", "tp"),
            P("ep", "tp"),
            P("ep", "tp"),
            P("tp"),
            P("ep", "tp"),
            P("tp"),
            P("tp", None),
            P("ep", None),
            P(),
            P("ep", None),
            P("ep", None),
            P("ep", None, "tp"),
            P("ep", None, "tp"),
            P("ep", None, "tp"),
        ),
        out_specs=(P(("ep", "tp"), None), P("ep", "tp")),
        check_vma=False,
    )
```

```python
import functools

import jax
import jax.numpy as jnp
from jax import lax
from jax.experimental import pallas as pl
from jax.experimental.pallas import tpu as pltpu
from jax.sharding import PartitionSpec as P

HEAD_DIM = 128
CHUNK = 64
MESH = pl.DeviceIdType.MESH
F32 = jnp.float32
BF16 = jnp.bfloat16


def flip(i, k):
    b = 1
    while b <= k:
        if k & b:
            i = i + b - 2 * b * lax.rem(lax.div(i, b), 2)
        b *= 2
    return i


def kernel(
    E, T, cap, near, slots, each, plan,
    q_hbm, f_hbm, v_hbm, o_hbm, gap_ref, extra_hbm, hscale_ref,
    mixw_hbm, tok_ref, escale_ref, routes_ref, scores_ref,
    gate_hbm, up_hbm, down_hbm,
    mix_out, exp_out,
    q_ref, f_ref, v_ref, o_ref, extra_ref,
    gate, up, down, mixw,
    ncols, dmat, wmat, outgoing, nearout, feats, hidden, part, precv, xsend, xrecv, fin, ret,
    qs, ks, run, qg, rec, ist, idec, est, bst, bdec, psum, pdec, ksend, krecv, csend, crecv, tsend, trecv,
    mhid, mpart, mprecv, mxsend, mxrecv,
    wsem, send_sem, recv_sem,
):
    me = lax.axis_index("ep")
    t = lax.axis_index("tp")
    G = T // 2
    g, c = lax.div(t, 2), lax.rem(t, 2)
    oc = 1 - c
    tokens, width = q_ref.shape
    heads = width // HEAD_DIM
    Dl = outgoing.shape[1]
    FFl = hidden.shape[1]

    loads = [
        pltpu.make_async_copy(src, dst, wsem.at[i])
        for i, (src, dst) in enumerate(
            (
                (f_hbm, f_ref), (extra_hbm, extra_ref), (q_hbm, q_ref), (v_hbm, v_ref),
                (gate_hbm, gate), (up_hbm, up), (down_hbm, down),
                (o_hbm, o_ref), (mixw_hbm, mixw),
            )
        )
    ]

    barrier = pltpu.get_barrier_semaphore()
    for k in range(1, E):
        pl.semaphore_signal(barrier, inc=1, device_id=(flip(me, k), t), device_id_type=MESH)
    pl.semaphore_signal(barrier, inc=1, device_id=(me, 2 * g + oc), device_id_type=MESH)
    for j in range(1, G):
        pl.semaphore_signal(
            barrier, inc=1, device_id=(me, 2 * flip(g, j) + c), device_id_type=MESH
        )

    for load in loads:
        load.start()

    used = [0]

    def remote(src, dst, device):
        slot = used[0]
        used[0] += 1
        return pltpu.make_async_remote_copy(
            src_ref=src, dst_ref=dst, send_sem=send_sem.at[slot], recv_sem=recv_sem.at[slot],
            device_id=device, device_id_type=MESH,
        )

    sent = []
    partner = (me, 2 * g + oc)

    def launch(copy):
        copy.start()
        sent.append(copy)
        return copy

    x = tok_ref[...].astype(F32)
    mean = jnp.mean(x, axis=-1, keepdims=True)
    centred = x - mean
    inv = lax.rsqrt(jnp.mean(centred * centred, axis=-1, keepdims=True) + 1e-05)

    def normed(cols):
        return ((tok_ref[:, cols].astype(F32) - mean) * inv * escale_ref[:, cols]).astype(BF16)

    ntok = tok_ref.shape[0]
    ek = lax.broadcasted_iota(jnp.int32, (E, ntok), 0) ^ me
    first, second = routes_ref[0:1, :] == ek, routes_ref[1:2, :] == ek
    named = jnp.where(first | second, 1.0, 0.0)
    earlier = jnp.where(
        lax.broadcasted_iota(jnp.int32, (ntok, ntok), 0)
        < lax.broadcasted_iota(jnp.int32, (ntok, ntok), 1), 1.0, 0.0
    ).astype(BF16)
    position = jnp.dot(named.astype(BF16), earlier, preferred_element_type=F32)
    place = jnp.where(first | second, position, -1.0).astype(jnp.int32)
    rows = lax.broadcasted_iota(jnp.int32, (cap, ntok), 0)

    z = lax.div(me, 2)
    Z = E // 2
    swap = E == 8
    inner = lax.rem(z + lax.div(z, 2), 2) if swap else 0

    def by_side(a, b):
        return a + inner * (b - a)

    def peer(a, b):
        return flip(me, a) if a == b else by_side(flip(me, a), flip(me, b))

    def row_of(table, i):
        a, b = (to[i] for to in slots["to"])
        outside, inside = table[a:a + 1, :], table[b:b + 1, :]
        return outside if a == b else jnp.where(inner == 1, inside, outside)

    def cross(i):
        return (i - near) % 2 if swap else 0

    def choose(i):
        dmat[i * cap:(i + 1) * cap, :] = jnp.where(rows == row_of(place, i), 1.0, 0.0).astype(BF16)

    for i in range(near, E):
        choose(i)
    own = normed(pl.ds(pl.multiple_of(t * Dl, 128), Dl))
    outgoing[...] = jnp.dot(
        dmat[near * cap:, :], own, preferred_element_type=F32
    ).astype(BF16)

    dispatch = {}

    far_base, back_base = used[0], used[0] + E
    used[0] += 2 * E

    def placed(src, dst, position, device, send, base):
        block = pl.ds(pl.multiple_of(position * cap, 16), cap)
        return pltpu.make_async_remote_copy(
            src_ref=src, dst_ref=dst(block), send_sem=send_sem.at[base + send],
            recv_sem=recv_sem.at[base + position], device_id=device, device_id_type=MESH,
        )

    def far_block(block):
        return feats.at[c, g, block]

    def ret_block(block):
        return ret.at[block]

    def send_far(i):
        a, b = (to[i] for to in slots["to"])
        to = near + 2 * inner + (i - near) // 2 if swap else i
        src = outgoing.at[pl.ds((i - near) * cap, cap)]
        launch(placed(src, far_block, to, (peer(a, b), t), i, far_base))

    def far_arrived(i):
        src = outgoing.at[pl.ds((i - near) * cap, cap)]
        placed(src, far_block, i, partner, i, far_base).wait_recv()

    def send_back(i):
        a, b = (source[i] for source in slots["from"])
        to = near + inner + 2 * cross(i) if swap and i >= near else i
        src = fin.at[pl.ds(i * cap, cap)]
        launch(placed(src, ret_block, to, (peer(a, b), t), i, back_base))

    def back_arrived(i):
        placed(fin.at[pl.ds(i * cap, cap)], ret_block, i, partner, i, back_base).wait_recv()

    def send_near(i):
        dispatch[i] = launch(remote(
            nearout.at[:, pl.ds((i - 1) * cap, cap)],
            feats.at[c, :, pl.ds(i * cap, cap)], (flip(me, i), t),
        ))

    pl.semaphore_wait(barrier, E - 1 + 1 + G - 1)

    def far_out(p):
        for i in range(p * each, (p + 1) * each):
            send_far(i)

    def near_out(p):
        for i in range(max(1, p * each), (p + 1) * each):
            send_near(i)

    def near_prepare():
        for i in range(near):
            choose(i)
        for d in range(T):
            ncols[d % 2, d // 2] = normed(slice(d * Dl, (d + 1) * Dl))
        for j in range(G):
            nearout[j] = jnp.dot(
                dmat[cap:near * cap, :], ncols[c, j], preferred_element_type=F32
            ).astype(BF16)

    def local_features():
        for d in range(T):
            feats[d % 2, d // 2, 0:cap, :] = jnp.dot(
                dmat[0:cap, :], ncols[d % 2, d // 2], preferred_element_type=F32
            ).astype(BF16)

    r_i = lax.broadcasted_iota(jnp.int32, (CHUNK, CHUNK), 0)
    c_i = lax.broadcasted_iota(jnp.int32, (CHUNK, CHUNK), 1)
    causal = r_i >= c_i
    nchunks = tokens // CHUNK

    def head_local(h, _):
        lanes = pl.ds(pl.multiple_of(h * HEAD_DIM, HEAD_DIM), HEAD_DIM)
        state = jnp.zeros((HEAD_DIM, HEAD_DIM), F32)
        before = jnp.zeros((1, HEAD_DIM), F32)
        for n in range(nchunks):
            rs = slice(n * CHUNK, (n + 1) * CHUNK)
            r = run[rs, lanes]
            total = r[CHUNK - 1:CHUNK, :]
            qd = qs[rs, lanes] * jnp.exp(r)
            key = ks[rs, lanes]
            kd = (key * jnp.exp(-r)).astype(BF16)
            kst = (key * jnp.exp(total - r)).astype(BF16)
            val = v_ref[rs, lanes]
            qd_b = qd.astype(BF16)
            scores = lax.dot_general(
                qd_b, kd, (((1,), (1,)), ((), ())), preferred_element_type=F32
            )
            scores = jnp.where(causal, scores, 0.0).astype(BF16)
            out = jnp.dot(scores, val, preferred_element_type=F32)
            if n:
                out += lax.dot_general(
                    qd_b, state.astype(BF16), (((1,), (1,)), ((), ())),
                    preferred_element_type=F32,
                )
            rec[rs, lanes] = out
            qg[rs, lanes] = (qd * jnp.exp(before)).astype(BF16)
            state = state * jnp.exp(total) + lax.dot_general(
                val, kst, (((0,), (0,)), ((), ())), preferred_element_type=F32
            )
            before = before + total
        ist[h] = state
        idec[h] = jnp.broadcast_to(jnp.exp(before), (16, HEAD_DIM))
        return 0

    odd = lax.rem(me, 2) == 1
    pair = remote(ksend, krecv, (flip(me, 1), t))
    scan = E == 8
    if scan:
        climb = remote(tsend, trecv, (lax.rem(me + 2, E), t))
        hand = [remote(csend, crecv, (lax.rem(me + 2 + 2 * i, E), t)) for i in range(2)]
    chain = remote(csend, crecv, (lax.rem(me + 2, E), t)) if Z > 1 and not scan else None

    def recurrence():
        for load in loads[:4]:
            load.wait()
        closing = gap_ref[...] * jax.nn.sigmoid(-f_ref[...].astype(F32))
        ks[...] = closing
        logd = jnp.log1p(-closing) + extra_ref[...]
        qs[...] = jax.nn.silu(q_ref[...].astype(F32))
        tri = jnp.where(causal, 1.0, 0.0).astype(F32)
        for n in range(nchunks):
            run[n * CHUNK:(n + 1) * CHUNK, :] = jnp.dot(
                tri, logd[n * CHUNK:(n + 1) * CHUNK, :], precision=lax.Precision.HIGHEST,
                preferred_element_type=F32,
            )

        lax.fori_loop(0, heads, head_local, 0)
        ksend[:, 0:HEAD_DIM, :] = ist[...].astype(BF16)
        ksend[:, HEAD_DIM:, :] = idec[...].astype(BF16)
        launch(pair)

    def pair_end():
        pair.wait_recv()
        s = krecv[:, 0:HEAD_DIM, :].astype(F32)
        d = krecv[:, HEAD_DIM:, :].astype(F32)
        bst[...] = jnp.where(odd, s, 0.0)
        bdec[...] = jnp.where(odd, d, 1.0)
        psum[...] = jnp.where(
            odd, idec[:, 0:1, :] * s + ist[...], d[:, 0:1, :] * ist[...] + s
        )
        pdec[...] = idec[...] * d

    def carry_in(carry):
        est[...] = bdec[:, 0:1, :] * carry + bst[...]

    def scan_step(i):
        if i == 0:
            @pl.when(lax.rem(z, 2) == 0)
            def _():
                est[...] = bst[...]
                tsend[:, 0:HEAD_DIM, :] = psum[...].astype(BF16)
                tsend[:, HEAD_DIM:, :] = pdec[...].astype(BF16)
                climb.start()
        elif i == 1:
            @pl.when(lax.rem(z, 2) == 1)
            def _():
                climb.wait_recv()

            @pl.when(z == 1)
            def _():
                carry = trecv[:, 0:HEAD_DIM, :].astype(F32)
                carry_in(carry)
                csend[...] = (pdec[:, 0:1, :] * carry + psum[...]).astype(BF16)
                hand[0].start()
                hand[1].start()
        elif i == 2:
            @pl.when(z == 2)
            def _():
                hand[0].wait_recv()
                carry_in(crecv[...].astype(F32))

            @pl.when(z == 3)
            def _():
                hand[1].wait_recv()
                decay = trecv[:, HEAD_DIM:HEAD_DIM + 1, :].astype(F32)
                carry_in(decay * crecv[...].astype(F32) + trecv[:, 0:HEAD_DIM, :].astype(F32))

    def chain_step(i):
        if scan:
            scan_step(i)
            return

        @pl.when(z == i)
        def _():
            if i:
                chain.wait_recv()
                carry = crecv[...].astype(F32)
                est[...] = bdec[:, 0:1, :] * carry + bst[...]
                if i + 1 < Z:
                    csend[...] = (pdec[:, 0:1, :] * carry + psum[...]).astype(BF16)
            else:
                est[...] = bst[...]
                if i + 1 < Z:
                    csend[...] = psum[...].astype(BF16)
            if i + 1 < Z:
                chain.start()

    def weigh():
        w0 = jax.nn.sigmoid(scores_ref[0:1, :] - scores_ref[1:2, :])
        weight = jnp.where(first, w0, jnp.where(second, 1.0 - w0, 0.0))
        for i in range(E):
            wmat[i * cap:(i + 1) * cap, :] = jnp.where(
                rows == row_of(place, i), row_of(weight, i), 0.0
            ).astype(BF16)

    ag_partner, ag_cross, rs_partner, rs_cross = {}, {}, {}, {}

    def unit(p):
        return p * each, each

    def piece_rows(p):
        return pl.ds(p * each * cap, each * cap)

    def gather_start(p):
        a, n = unit(p)
        lo = max(a, 1)
        if lo == a + n:
            return
        for i in range(lo, a + n):
            dispatch[i].wait_recv() if i < near else far_arrived(i)
        if a < near:
            rr = pl.ds(lo * cap, (a + n - lo) * cap)
            ag_partner[p, 0] = launch(remote(feats.at[c, :, rr], feats.at[c, :, rr], partner))
            return
        rr = piece_rows(p)
        for j in range(1, G):
            ag_cross[p, j] = launch(
                remote(feats.at[c, g, rr], feats.at[c, g, rr], (me, 2 * flip(g, j) + c))
            )
        ag_partner[p, 0] = launch(remote(feats.at[c, g, rr], feats.at[c, g, rr], partner))

    def gather_relay(p):
        rr = piece_rows(p)
        for j in range(1, G):
            ag_cross[p, j].wait_recv()
            gj = flip(g, j)
            ag_partner[p, j] = launch(remote(feats.at[c, gj, rr], feats.at[c, gj, rr], partner))

    def gather_end(p):
        for j in range(G):
            if (p, j) in ag_partner:
                ag_partner[p, j].wait_recv()

    tile = min(256, FFl)

    def experts(*units):
        if not rs_partner:
            for load in loads[4:7]:
                load.wait()
        for p in units:
            gather_end(p)
        n = len(units) * each
        rs = slice(units[0] * each * cap, (units[-1] + 1) * each * cap)
        for i in range(FFl // tile):
            cc = slice(i * tile, (i + 1) * tile)
            ga = jnp.zeros((n * cap, tile), F32)
            ua = jnp.zeros((n * cap, tile), F32)
            for d in range(T):
                xs = feats[d % 2, d // 2, rs, :]
                ga += jnp.dot(xs, gate[d * Dl:(d + 1) * Dl, cc], preferred_element_type=F32)
                ua += jnp.dot(xs, up[d * Dl:(d + 1) * Dl, cc], preferred_element_type=F32)
            hidden[rs, cc] = (jax.nn.silu(ga) * ua).astype(BF16)

        def down_group(cls, gg):
            ff = pl.ds(pl.multiple_of((2 * gg + cls) * Dl, 128), Dl)
            part[cls, gg, rs, :] = lax.dot_general(
                hidden[rs, :], down[ff, :], (((1,), (1,)), ((), ())),
                preferred_element_type=F32,
            ).astype(BF16)

        for gg in range(G):
            down_group(oc, gg)
        for p in units:
            rr = piece_rows(p)
            rs_partner[p] = launch(remote(part.at[oc, :, rr], precv.at[:, rr], partner))
        for gg in range(G):
            down_group(c, gg)

    def scatter_cross(p):
        a, n = unit(p)
        rs = slice(a * cap, (a + n) * cap)
        rr = piece_rows(p)
        rs_partner[p].wait_recv()
        for j in range(1, G):
            gj = flip(g, j)
            xsend[j - 1, rs, :] = (
                part[c, gj, rs, :].astype(F32) + precv[gj, rs, :].astype(F32)
            ).astype(BF16)
            rs_cross[p, j] = launch(
                remote(xsend.at[j - 1, rr], xrecv.at[j - 1, rr], (me, 2 * gj + c))
            )

    def give_back(p):
        a, n = unit(p)
        rs = slice(a * cap, (a + n) * cap)
        total = part[c, g, rs, :].astype(F32) + precv[g, rs, :].astype(F32)
        for j in range(1, G):
            rs_cross[p, j].wait_recv()
            total += xrecv[j - 1, rs, :].astype(F32)
        fin[rs, :] = total.astype(BF16)
        for i in range(max(a, 1), a + n):
            send_back(i)
        if a == 0:
            ret[0:cap, :] = fin[0:cap, :]

    def mixer_end():
        for load in loads[7:]:
            load.wait()
        for h in range(heads):
            lanes = slice(h * HEAD_DIM, (h + 1) * HEAD_DIM)
            r = rec[:, lanes] + lax.dot_general(
                qg[:, lanes], est[h].astype(BF16), (((1,), (1,)), ((), ())),
                preferred_element_type=F32,
            )
            r = r * lax.rsqrt(jnp.mean(r * r, axis=-1, keepdims=True) + 1e-06)
            mhid[:, lanes] = (
                r * hscale_ref[:, lanes] * jax.nn.silu(o_ref[:, lanes].astype(F32))
            ).astype(BF16)
        R = mix_out.shape[0]
        wide = mixw.shape[1]
        step = min(512, wide)

        def one(i, _):
            cc = pl.ds(pl.multiple_of(i * step, step), step)
            y = jnp.dot(mhid[...], mixw[:, cc], preferred_element_type=F32).astype(BF16)
            for d in range(T):
                mpart[d % 2, d // 2, :, cc] = y[d * R:(d + 1) * R, :]
            return 0

        lax.fori_loop(0, wide // step, one, 0)
        rs_partner["m"] = launch(remote(mpart.at[oc], mprecv, partner))

    def mixer_cross():
        rs_partner["m"].wait_recv()
        for j in range(1, G):
            gj = flip(g, j)
            mxsend[j - 1] = (mpart[c, gj].astype(F32) + mprecv[gj].astype(F32)).astype(BF16)
            rs_cross["m", j] = launch(
                remote(mxsend.at[j - 1], mxrecv.at[j - 1], (me, 2 * gj + c))
            )

    def mixer_out():
        total = mpart[c, g].astype(F32) + mprecv[g].astype(F32)
        for j in range(1, G):
            rs_cross["m", j].wait_recv()
            total += mxrecv[j - 1].astype(F32)
        mix_out[...] = total.astype(BF16)

    def chain_rest(i):
        for i in range(i, Z):
            chain_step(i)

    steps = {
        "f": far_out, "n": near_out, "p": near_prepare, "l": local_features, "h": recurrence,
        "a": gather_start, "b": gather_relay, "c": experts, "d": scatter_cross, "e": give_back,
        "pair": pair_end, "chain": chain_step, "chains": chain_rest,
        "w": weigh, "mc": mixer_end, "md": mixer_cross, "me": mixer_out,
    }
    for step in plan:
        steps[step[0]](*step[1:])
    for i in range(1, E):
        back_arrived(i)
    exp_out[...] = lax.dot_general(
        wmat[...], ret[...], (((0,), (0,)), ((), ())), preferred_element_type=F32
    ).astype(BF16)
    for copy in sent:
        copy.wait_send()
    if scan:
        @pl.when(lax.rem(z, 2) == 0)
        def _():
            climb.wait_send()

        @pl.when(z == 1)
        def _():
            hand[0].wait_send()
            hand[1].wait_send()

    if chain is not None:
        @pl.when(me + 2 < E)
        def _():
            chain.wait_send()


STEPS = (
    "f 4", "f 5", "f 6", "f 7", "p", "n 1", "h", "n 2", "l", "c 0", "a 4", "d 0",
    "a 1", "c 1", "a 5", "b 4", "pair", "chain 0", "n 3", "d 1", "c 4", "b 5", "a 2", "a 6",
    "d 4", "chain 1", "a 7",
    "c 5", "d 5", "a 3", "e 0", "e 1", "c 2 3", "d 2", "d 3", "e 4", "chain 2", "b 6", "b 7",
    "c 6 7", "d 6", "d 7", "e 5", "chains 3", "mc", "e 2", "e 6", "md", "e 7", "w", "e 3",
    "me",
)


def make_plan():
    return [(s[0], *(int(i) for i in s[1:])) for s in map(str.split, STEPS)]


def body(E, T, q, f, v, o, gap, extra, hscale, mixw, tok, escale, routes, scores, gate, up, down):
    tokens, width = q.shape
    ntok, D = tok.shape
    heads = width // HEAD_DIM
    G = T // 2
    cap = -(-(3 * ntok // E) // 16) * 16
    S = E * cap
    Dl = D // T
    FFl = gate.shape[2]
    R = tokens // T
    near = E // 2
    each = E // 8
    close, far = list(range(near)), list(range(near, E))
    plain = (close + far, close + far)
    slots = {"to": plain, "from": plain}
    if E == 8:
        slots["to"] = (close + [6, 4, 7, 5], close + [4, 6, 5, 7])
        slots["from"] = (close + [6, 7, 4, 5], close + [4, 5, 6, 7])
    copies = 3 * E + 4 + 8 * (G - 1 + G + 1 + G - 1) + G
    vm = pl.BlockSpec(memory_space=pltpu.VMEM)
    anyspace = pl.BlockSpec(memory_space=pl.ANY)
    V = pltpu.VMEM
    scratch = [
        V(q.shape, BF16), V(q.shape, BF16), V(q.shape, BF16), V(q.shape, BF16), V(q.shape, F32),
        V((D, FFl), BF16), V((D, FFl), BF16), V((D, FFl), BF16), V(mixw.shape, BF16),
        V((2, G, ntok, Dl), BF16), V((S, ntok), BF16), V((S, ntok), BF16),
        V(((E - near) * cap, Dl), BF16), V((G, (near - 1) * cap, Dl), BF16),
        V((2, G, S, Dl), BF16), V((S, FFl), BF16), V((2, G, S, Dl), BF16), V((G, S, Dl), BF16),
        V((max(G - 1, 1), S, Dl), BF16), V((max(G - 1, 1), S, Dl), BF16),
        V((S, Dl), BF16), V((S, Dl), BF16),
        V((tokens, width), F32), V((tokens, width), F32), V((tokens, width), F32),
        V((tokens, width), BF16), V((tokens, width), F32),
        V((heads, HEAD_DIM, HEAD_DIM), F32), V((heads, 16, HEAD_DIM), F32),
        V((heads, HEAD_DIM, HEAD_DIM), F32),
        V((heads, HEAD_DIM, HEAD_DIM), F32), V((heads, 16, HEAD_DIM), F32),
        V((heads, HEAD_DIM, HEAD_DIM), F32), V((heads, 16, HEAD_DIM), F32),
        V((heads, HEAD_DIM + 16, HEAD_DIM), BF16), V((heads, HEAD_DIM + 16, HEAD_DIM), BF16),
        V((heads, HEAD_DIM, HEAD_DIM), BF16), V((heads, HEAD_DIM, HEAD_DIM), BF16),
        V((heads, HEAD_DIM + 16, HEAD_DIM), BF16), V((heads, HEAD_DIM + 16, HEAD_DIM), BF16),
        V((tokens, width), BF16), V((2, G, R, D), BF16), V((G, R, D), BF16),
        V((max(G - 1, 1), R, D), BF16), V((max(G - 1, 1), R, D), BF16),
        pltpu.SemaphoreType.DMA((9,)),
        pltpu.SemaphoreType.DMA((copies,)),
        pltpu.SemaphoreType.DMA((copies,)),
    ]
    return pl.pallas_call(
        functools.partial(kernel, E, T, cap, near, slots, each, make_plan()),
        out_shape=(
            pltpu.VMEM((R, D), BF16),
            pltpu.VMEM((ntok, Dl), BF16),
        ),
        in_specs=(
            [anyspace] * 4 + [vm, anyspace, vm, anyspace] + [vm] * 4 + [anyspace] * 3
        ),
        out_specs=(vm, vm),
        scratch_shapes=scratch,
        compiler_params=pltpu.CompilerParams(
            collective_id=0, has_side_effects=True, vmem_limit_bytes=60 * 1024 * 1024
        ),
    )(
        q, f, v, o, gap[None], extra, hscale[None], mixw, tok, escale[None],
        routes.T, scores.T, gate[0], up[0], down[0],
    )


def solution(mesh):
    E, T = mesh.shape["ep"], mesh.shape["tp"]
    return jax.shard_map(
        functools.partial(body, E, T),
        mesh=mesh,
        in_specs=(
            P("ep", "tp"),
            P("ep", "tp"),
            P("ep", "tp"),
            P("ep", "tp"),
            P("tp"),
            P("ep", "tp"),
            P("tp"),
            P("tp", None),
            P("ep", None),
            P(),
            P("ep", None),
            P("ep", None),
            P("ep", None, "tp"),
            P("ep", None, "tp"),
            P("ep", None, "tp"),
        ),
        out_specs=(P(("ep", "tp"), None), P("ep", "tp")),
        check_vma=False,
    )
```

```python
import functools

import jax
import jax.numpy as jnp
from jax import lax
from jax.experimental import pallas as pl
from jax.experimental.pallas import tpu as pltpu
from jax.sharding import PartitionSpec as P

HEAD_DIM = 128
CHUNK = 64
POOL = 24
MESH = pl.DeviceIdType.MESH
F32 = jnp.float32
BF16 = jnp.bfloat16


def flip(i, k):
    b = 1
    while b <= k:
        if k & b:
            i = i + b - 2 * b * lax.rem(lax.div(i, b), 2)
        b *= 2
    return i


def kernel(
    E, T, cap, near, slots, each, plan,
    q_hbm, f_hbm, v_hbm, o_hbm, gap_ref, extra_hbm, hscale_ref,
    mixw_hbm, tok_ref, escale_ref, routes_ref, scores_ref,
    gate_hbm, up_hbm, down_hbm,
    mix_out, exp_out,
    q_ref, f_ref, v_ref, o_ref, extra_ref,
    gate, up, down, mixw,
    ncols, dmat, wmat, outgoing, nearout, feats, hidden, part, precv, xsend, xrecv, fin, ret,
    qs, ks, run, qg, rec, ist, idec, est, bst, bdec, psum, pdec, ksend, krecv, csend, crecv, tsend, trecv,
    mhid, mpart, mprecv, mxsend, mxrecv,
    wsem, send_sem, recv_sem,
):
    me = lax.axis_index("ep")
    t = lax.axis_index("tp")
    G = T // 2
    g, c = lax.div(t, 2), lax.rem(t, 2)
    oc = 1 - c
    tokens, width = q_ref.shape
    heads = width // HEAD_DIM
    Dl = outgoing.shape[1]
    FFl = hidden.shape[1]

    loads = [
        pltpu.make_async_copy(src, dst, wsem.at[i])
        for i, (src, dst) in enumerate(
            (
                (f_hbm, f_ref), (extra_hbm, extra_ref), (q_hbm, q_ref), (v_hbm, v_ref),
                (gate_hbm, gate), (up_hbm, up), (down_hbm, down),
                (o_hbm, o_ref), (mixw_hbm, mixw),
            )
        )
    ]

    barrier = pltpu.get_barrier_semaphore()
    for k in range(1, E):
        pl.semaphore_signal(barrier, inc=1, device_id=(flip(me, k), t), device_id_type=MESH)
    pl.semaphore_signal(barrier, inc=1, device_id=(me, 2 * g + oc), device_id_type=MESH)
    for j in range(1, G):
        pl.semaphore_signal(
            barrier, inc=1, device_id=(me, 2 * flip(g, j) + c), device_id_type=MESH
        )

    for load in loads:
        load.start()

    used = [0]
    sent = []
    idle = list(range(POOL))

    def send_slot():
        if idle:
            return idle.pop(0)
        copy, slot = sent.pop(0)
        copy.wait_send()
        return slot

    def remote(src, dst, device, held=None):
        recv, slot = used[0], send_slot() if held is None else held
        used[0] += 1
        copy = pltpu.make_async_remote_copy(
            src_ref=src, dst_ref=dst, send_sem=send_sem.at[slot], recv_sem=recv_sem.at[recv],
            device_id=device, device_id_type=MESH,
        )
        return copy, slot

    def launch(made):
        made[0].start()
        sent.append(made)
        return made[0]

    partner = (me, 2 * g + oc)

    x = tok_ref[...].astype(F32)
    mean = jnp.mean(x, axis=-1, keepdims=True)
    centred = x - mean
    inv = lax.rsqrt(jnp.mean(centred * centred, axis=-1, keepdims=True) + 1e-05)

    def normed(cols):
        return ((tok_ref[:, cols].astype(F32) - mean) * inv * escale_ref[:, cols]).astype(BF16)

    ntok = tok_ref.shape[0]
    ek = lax.broadcasted_iota(jnp.int32, (E, ntok), 0) ^ me
    first, second = routes_ref[0:1, :] == ek, routes_ref[1:2, :] == ek
    named = jnp.where(first | second, 1.0, 0.0)
    earlier = jnp.where(
        lax.broadcasted_iota(jnp.int32, (ntok, ntok), 0)
        < lax.broadcasted_iota(jnp.int32, (ntok, ntok), 1), 1.0, 0.0
    ).astype(BF16)
    position = jnp.dot(named.astype(BF16), earlier, preferred_element_type=F32)
    place = jnp.where(first | second, position, -1.0).astype(jnp.int32)
    rows = lax.broadcasted_iota(jnp.int32, (cap, ntok), 0)

    z = lax.div(me, 2)
    Z = E // 2
    swap = E == 8
    inner = lax.rem(z + lax.div(z, 2), 2) if swap else 0

    def by_side(a, b):
        return a + inner * (b - a)

    def peer(a, b):
        return flip(me, a) if a == b else by_side(flip(me, a), flip(me, b))

    def row_of(table, i):
        a, b = (to[i] for to in slots["to"])
        outside, inside = table[a:a + 1, :], table[b:b + 1, :]
        return outside if a == b else jnp.where(inner == 1, inside, outside)

    def cross(i):
        return (i - near) % 2 if swap else 0

    def choose(i):
        dmat[i * cap:(i + 1) * cap, :] = jnp.where(rows == row_of(place, i), 1.0, 0.0).astype(BF16)

    for i in range(near, E):
        choose(i)
    own = normed(pl.ds(pl.multiple_of(t * Dl, 128), Dl))
    outgoing[...] = jnp.dot(
        dmat[near * cap:, :], own, preferred_element_type=F32
    ).astype(BF16)

    dispatch = {}

    far_base, back_base = used[0] - near, used[0] + E - near - 1
    used[0] += E - near + E - 1

    def placed(src, dst, position, device, slot, base):
        block = pl.ds(pl.multiple_of(position * cap, 16), cap)
        copy = pltpu.make_async_remote_copy(
            src_ref=src, dst_ref=dst(block), send_sem=send_sem.at[slot],
            recv_sem=recv_sem.at[base + position], device_id=device, device_id_type=MESH,
        )
        return copy, slot

    def far_block(block):
        return feats.at[c, g, block]

    def ret_block(block):
        return ret.at[block]

    def send_far(i):
        a, b = (to[i] for to in slots["to"])
        to = near + 2 * inner + (i - near) // 2 if swap else i
        src = outgoing.at[pl.ds((i - near) * cap, cap)]
        launch(placed(src, far_block, to, (peer(a, b), t), send_slot(), far_base))

    def far_arrived(i):
        src = outgoing.at[pl.ds((i - near) * cap, cap)]
        placed(src, far_block, i, partner, 0, far_base)[0].wait_recv()

    def send_back(i):
        a, b = (source[i] for source in slots["from"])
        to = near + inner + 2 * cross(i) if swap and i >= near else i
        src = fin.at[pl.ds(i * cap, cap)]
        launch(placed(src, ret_block, to, (peer(a, b), t), send_slot(), back_base))

    def back_arrived(i):
        placed(fin.at[pl.ds(i * cap, cap)], ret_block, i, partner, 0, back_base)[0].wait_recv()

    def send_near(i):
        dispatch[i] = launch(remote(
            nearout.at[:, pl.ds((i - 1) * cap, cap)],
            feats.at[c, :, pl.ds(i * cap, cap)], (flip(me, i), t),
        ))

    pl.semaphore_wait(barrier, E - 1 + 1 + G - 1)

    def far_out(p):
        for i in range(p * each, (p + 1) * each):
            send_far(i)

    def near_out(p):
        for i in range(max(1, p * each), (p + 1) * each):
            send_near(i)

    def near_prepare():
        for i in range(near):
            choose(i)
        for d in range(T):
            ncols[d % 2, d // 2] = normed(slice(d * Dl, (d + 1) * Dl))
        for j in range(G):
            nearout[j] = jnp.dot(
                dmat[cap:near * cap, :], ncols[c, j], preferred_element_type=F32
            ).astype(BF16)

    def local_features():
        for d in range(T):
            feats[d % 2, d // 2, 0:cap, :] = jnp.dot(
                dmat[0:cap, :], ncols[d % 2, d // 2], preferred_element_type=F32
            ).astype(BF16)

    r_i = lax.broadcasted_iota(jnp.int32, (CHUNK, CHUNK), 0)
    c_i = lax.broadcasted_iota(jnp.int32, (CHUNK, CHUNK), 1)
    causal = r_i >= c_i
    nchunks = tokens // CHUNK

    def head_local(h, _):
        lanes = pl.ds(pl.multiple_of(h * HEAD_DIM, HEAD_DIM), HEAD_DIM)
        state = jnp.zeros((HEAD_DIM, HEAD_DIM), F32)
        before = jnp.zeros((1, HEAD_DIM), F32)
        for n in range(nchunks):
            rs = slice(n * CHUNK, (n + 1) * CHUNK)
            r = run[rs, lanes]
            total = r[CHUNK - 1:CHUNK, :]
            qd = qs[rs, lanes] * jnp.exp(r)
            key = ks[rs, lanes]
            kd = (key * jnp.exp(-r)).astype(BF16)
            kst = (key * jnp.exp(total - r)).astype(BF16)
            val = v_ref[rs, lanes]
            qd_b = qd.astype(BF16)
            scores = lax.dot_general(
                qd_b, kd, (((1,), (1,)), ((), ())), preferred_element_type=F32
            )
            scores = jnp.where(causal, scores, 0.0).astype(BF16)
            out = jnp.dot(scores, val, preferred_element_type=F32)
            if n:
                out += lax.dot_general(
                    qd_b, state.astype(BF16), (((1,), (1,)), ((), ())),
                    preferred_element_type=F32,
                )
            rec[rs, lanes] = out
            qg[rs, lanes] = (qd * jnp.exp(before)).astype(BF16)
            state = state * jnp.exp(total) + lax.dot_general(
                val, kst, (((0,), (0,)), ((), ())), preferred_element_type=F32
            )
            before = before + total
        ist[h] = state
        idec[h] = jnp.broadcast_to(jnp.exp(before), (16, HEAD_DIM))
        return 0

    odd = lax.rem(me, 2) == 1
    pair = remote(ksend, krecv, (flip(me, 1), t))
    scan = E == 8
    if scan:
        climb = remote(tsend, trecv, (lax.rem(me + 2, E), t), POOL)[0]
        hand = [
            remote(csend, crecv, (lax.rem(me + 2 + 2 * i, E), t), POOL + 1 + i)[0]
            for i in range(2)
        ]
    chain = None
    if Z > 1 and not scan:
        chain = remote(csend, crecv, (lax.rem(me + 2, E), t), POOL)[0]

    def recurrence():
        for load in loads[:4]:
            load.wait()
        closing = gap_ref[...] * jax.nn.sigmoid(-f_ref[...].astype(F32))
        ks[...] = closing
        logd = jnp.log1p(-closing) + extra_ref[...]
        qs[...] = jax.nn.silu(q_ref[...].astype(F32))
        tri = jnp.where(causal, 1.0, 0.0).astype(F32)
        for n in range(nchunks):
            run[n * CHUNK:(n + 1) * CHUNK, :] = jnp.dot(
                tri, logd[n * CHUNK:(n + 1) * CHUNK, :], precision=lax.Precision.HIGHEST,
                preferred_element_type=F32,
            )

        lax.fori_loop(0, heads, head_local, 0)
        ksend[:, 0:HEAD_DIM, :] = ist[...].astype(BF16)
        ksend[:, HEAD_DIM:, :] = idec[...].astype(BF16)
        launch(pair)

    def pair_end():
        pair[0].wait_recv()
        s = krecv[:, 0:HEAD_DIM, :].astype(F32)
        d = krecv[:, HEAD_DIM:, :].astype(F32)
        bst[...] = jnp.where(odd, s, 0.0)
        bdec[...] = jnp.where(odd, d, 1.0)
        psum[...] = jnp.where(
            odd, idec[:, 0:1, :] * s + ist[...], d[:, 0:1, :] * ist[...] + s
        )
        pdec[...] = idec[...] * d

    def carry_in(carry):
        est[...] = bdec[:, 0:1, :] * carry + bst[...]

    def scan_step(i):
        if i == 0:
            @pl.when(lax.rem(z, 2) == 0)
            def _():
                est[...] = bst[...]
                tsend[:, 0:HEAD_DIM, :] = psum[...].astype(BF16)
                tsend[:, HEAD_DIM:, :] = pdec[...].astype(BF16)
                climb.start()
        elif i == 1:
            @pl.when(lax.rem(z, 2) == 1)
            def _():
                climb.wait_recv()

            @pl.when(z == 1)
            def _():
                carry = trecv[:, 0:HEAD_DIM, :].astype(F32)
                carry_in(carry)
                csend[...] = (pdec[:, 0:1, :] * carry + psum[...]).astype(BF16)
                hand[0].start()
                hand[1].start()
        elif i == 2:
            @pl.when(z == 2)
            def _():
                hand[0].wait_recv()
                carry_in(crecv[...].astype(F32))

            @pl.when(z == 3)
            def _():
                hand[1].wait_recv()
                decay = trecv[:, HEAD_DIM:HEAD_DIM + 1, :].astype(F32)
                carry_in(decay * crecv[...].astype(F32) + trecv[:, 0:HEAD_DIM, :].astype(F32))

    def chain_step(i):
        if scan:
            scan_step(i)
            return

        @pl.when(z == i)
        def _():
            if i:
                chain.wait_recv()
                carry = crecv[...].astype(F32)
                est[...] = bdec[:, 0:1, :] * carry + bst[...]
                if i + 1 < Z:
                    csend[...] = (pdec[:, 0:1, :] * carry + psum[...]).astype(BF16)
            else:
                est[...] = bst[...]
                if i + 1 < Z:
                    csend[...] = psum[...].astype(BF16)
            if i + 1 < Z:
                chain.start()

    def weigh():
        w0 = jax.nn.sigmoid(scores_ref[0:1, :] - scores_ref[1:2, :])
        weight = jnp.where(first, w0, jnp.where(second, 1.0 - w0, 0.0))
        for i in range(E):
            wmat[i * cap:(i + 1) * cap, :] = jnp.where(
                rows == row_of(place, i), row_of(weight, i), 0.0
            ).astype(BF16)

    ag_partner, ag_cross, rs_partner, rs_cross = {}, {}, {}, {}

    def unit(p):
        return p * each, each

    def piece_rows(p):
        return pl.ds(p * each * cap, each * cap)

    def gather_start(p):
        a, n = unit(p)
        lo = max(a, 1)
        if lo == a + n:
            return
        for i in range(lo, a + n):
            dispatch[i].wait_recv() if i < near else far_arrived(i)
        if a < near:
            rr = pl.ds(lo * cap, (a + n - lo) * cap)
            ag_partner[p, 0] = launch(remote(feats.at[c, :, rr], feats.at[c, :, rr], partner))
            return
        rr = piece_rows(p)
        for j in range(1, G):
            ag_cross[p, j] = launch(
                remote(feats.at[c, g, rr], feats.at[c, g, rr], (me, 2 * flip(g, j) + c))
            )
        ag_partner[p, 0] = launch(remote(feats.at[c, g, rr], feats.at[c, g, rr], partner))

    def gather_relay(p):
        rr = piece_rows(p)
        for j in range(1, G):
            ag_cross[p, j].wait_recv()
            gj = flip(g, j)
            ag_partner[p, j] = launch(remote(feats.at[c, gj, rr], feats.at[c, gj, rr], partner))

    def gather_end(p):
        for j in range(G):
            if (p, j) in ag_partner:
                ag_partner[p, j].wait_recv()

    tile = min(256, FFl)

    def experts(*units):
        if not rs_partner:
            for load in loads[4:7]:
                load.wait()
        for p in units:
            gather_end(p)
        n = len(units) * each
        rs = slice(units[0] * each * cap, (units[-1] + 1) * each * cap)
        for i in range(FFl // tile):
            cc = slice(i * tile, (i + 1) * tile)
            ga = jnp.zeros((n * cap, tile), F32)
            ua = jnp.zeros((n * cap, tile), F32)
            for d in range(T):
                xs = feats[d % 2, d // 2, rs, :]
                ga += jnp.dot(xs, gate[d * Dl:(d + 1) * Dl, cc], preferred_element_type=F32)
                ua += jnp.dot(xs, up[d * Dl:(d + 1) * Dl, cc], preferred_element_type=F32)
            hidden[rs, cc] = (jax.nn.silu(ga) * ua).astype(BF16)

        def down_group(cls, gg):
            ff = pl.ds(pl.multiple_of((2 * gg + cls) * Dl, 128), Dl)
            part[cls, gg, rs, :] = lax.dot_general(
                hidden[rs, :], down[ff, :], (((1,), (1,)), ((), ())),
                preferred_element_type=F32,
            ).astype(BF16)

        for gg in range(G):
            down_group(oc, gg)
        for p in units:
            rr = piece_rows(p)
            rs_partner[p] = launch(remote(part.at[oc, :, rr], precv.at[:, rr], partner))
        for gg in range(G):
            down_group(c, gg)

    def scatter_cross(p):
        a, n = unit(p)
        rs = slice(a * cap, (a + n) * cap)
        rr = piece_rows(p)
        rs_partner[p].wait_recv()
        for j in range(1, G):
            gj = flip(g, j)
            xsend[j - 1, rs, :] = (
                part[c, gj, rs, :].astype(F32) + precv[gj, rs, :].astype(F32)
            ).astype(BF16)
            rs_cross[p, j] = launch(
                remote(xsend.at[j - 1, rr], xrecv.at[j - 1, rr], (me, 2 * gj + c))
            )

    def give_back(p):
        a, n = unit(p)
        rs = slice(a * cap, (a + n) * cap)
        total = part[c, g, rs, :].astype(F32) + precv[g, rs, :].astype(F32)
        for j in range(1, G):
            rs_cross[p, j].wait_recv()
            total += xrecv[j - 1, rs, :].astype(F32)
        fin[rs, :] = total.astype(BF16)
        for i in range(max(a, 1), a + n):
            send_back(i)
        if a == 0:
            ret[0:cap, :] = fin[0:cap, :]

    def mixer_end():
        for load in loads[7:]:
            load.wait()
        for h in range(heads):
            lanes = slice(h * HEAD_DIM, (h + 1) * HEAD_DIM)
            r = rec[:, lanes] + lax.dot_general(
                qg[:, lanes], est[h].astype(BF16), (((1,), (1,)), ((), ())),
                preferred_element_type=F32,
            )
            r = r * lax.rsqrt(jnp.mean(r * r, axis=-1, keepdims=True) + 1e-06)
            mhid[:, lanes] = (
                r * hscale_ref[:, lanes] * jax.nn.silu(o_ref[:, lanes].astype(F32))
            ).astype(BF16)
        R = mix_out.shape[0]
        wide = mixw.shape[1]
        step = min(512, wide)

        def one(i, _):
            cc = pl.ds(pl.multiple_of(i * step, step), step)
            y = jnp.dot(mhid[...], mixw[:, cc], preferred_element_type=F32).astype(BF16)
            for d in range(T):
                mpart[d % 2, d // 2, :, cc] = y[d * R:(d + 1) * R, :]
            return 0

        lax.fori_loop(0, wide // step, one, 0)
        rs_partner["m"] = launch(remote(mpart.at[oc], mprecv, partner))

    def mixer_cross():
        rs_partner["m"].wait_recv()
        for j in range(1, G):
            gj = flip(g, j)
            mxsend[j - 1] = (mpart[c, gj].astype(F32) + mprecv[gj].astype(F32)).astype(BF16)
            rs_cross["m", j] = launch(
                remote(mxsend.at[j - 1], mxrecv.at[j - 1], (me, 2 * gj + c))
            )

    def mixer_out():
        total = mpart[c, g].astype(F32) + mprecv[g].astype(F32)
        for j in range(1, G):
            rs_cross["m", j].wait_recv()
            total += mxrecv[j - 1].astype(F32)
        mix_out[...] = total.astype(BF16)

    def chain_rest(i):
        for i in range(i, Z):
            chain_step(i)

    steps = {
        "f": far_out, "n": near_out, "p": near_prepare, "l": local_features, "h": recurrence,
        "a": gather_start, "b": gather_relay, "c": experts, "d": scatter_cross, "e": give_back,
        "pair": pair_end, "chain": chain_step, "chains": chain_rest,
        "w": weigh, "mc": mixer_end, "md": mixer_cross, "me": mixer_out,
    }
    for step in plan:
        steps[step[0]](*step[1:])
    assert used[0] <= recv_sem.shape[0]
    for i in range(1, E):
        back_arrived(i)
    exp_out[...] = lax.dot_general(
        wmat[...], ret[...], (((0,), (0,)), ((), ())), preferred_element_type=F32
    ).astype(BF16)
    for copy, _ in sent:
        copy.wait_send()
    if scan:
        @pl.when(lax.rem(z, 2) == 0)
        def _():
            climb.wait_send()

        @pl.when(z == 1)
        def _():
            hand[0].wait_send()
            hand[1].wait_send()

    if chain is not None:
        @pl.when(me + 2 < E)
        def _():
            chain.wait_send()


STEPS = (
    "f 4", "f 5", "p", "n 1", "f 6", "f 7", "h", "n 2", "l", "c 0", "a 4", "d 0",
    "a 1", "c 1", "a 5", "b 4", "pair", "chain 0", "n 3", "d 1", "c 4", "b 5", "a 2", "a 6",
    "d 4", "a 7",
    "c 5", "chain 1", "d 5", "a 3", "e 0", "e 1", "c 2 3", "d 2", "d 3", "e 4", "chain 2", "b 6",
    "b 7", "c 6 7", "d 6", "d 7", "e 5", "chains 3", "mc", "e 2", "e 6", "md", "e 7", "w",
    "e 3", "me",
)


def make_plan():
    return [(s[0], *(int(i) for i in s[1:])) for s in map(str.split, STEPS)]


def body(E, T, q, f, v, o, gap, extra, hscale, mixw, tok, escale, routes, scores, gate, up, down):
    tokens, width = q.shape
    ntok, D = tok.shape
    heads = width // HEAD_DIM
    G = T // 2
    cap = -(-(3 * ntok // E) // 16) * 16
    S = E * cap
    Dl = D // T
    FFl = gate.shape[2]
    R = tokens // T
    near = E // 2
    each = E // 8
    close, far = list(range(near)), list(range(near, E))
    plain = (close + far, close + far)
    slots = {"to": plain, "from": plain}
    if E == 8:
        slots["to"] = (close + [6, 4, 7, 5], close + [4, 6, 5, 7])
        slots["from"] = (close + [6, 7, 4, 5], close + [4, 5, 6, 7])
    copies = 2 * E - near - 1 + near - 1 + 8 + 4 * (2 * G - 1) + 9 * G
    vm = pl.BlockSpec(memory_space=pltpu.VMEM)
    anyspace = pl.BlockSpec(memory_space=pl.ANY)
    V = pltpu.VMEM
    scratch = [
        V(q.shape, BF16), V(q.shape, BF16), V(q.shape, BF16), V(q.shape, BF16), V(q.shape, F32),
        V((D, FFl), BF16), V((D, FFl), BF16), V((D, FFl), BF16), V(mixw.shape, BF16),
        V((2, G, ntok, Dl), BF16), V((S, ntok), BF16), V((S, ntok), BF16),
        V(((E - near) * cap, Dl), BF16), V((G, (near - 1) * cap, Dl), BF16),
        V((2, G, S, Dl), BF16), V((S, FFl), BF16), V((2, G, S, Dl), BF16), V((G, S, Dl), BF16),
        V((max(G - 1, 1), S, Dl), BF16), V((max(G - 1, 1), S, Dl), BF16),
        V((S, Dl), BF16), V((S, Dl), BF16),
        V((tokens, width), F32), V((tokens, width), F32), V((tokens, width), F32),
        V((tokens, width), BF16), V((tokens, width), F32),
        V((heads, HEAD_DIM, HEAD_DIM), F32), V((heads, 16, HEAD_DIM), F32),
        V((heads, HEAD_DIM, HEAD_DIM), F32),
        V((heads, HEAD_DIM, HEAD_DIM), F32), V((heads, 16, HEAD_DIM), F32),
        V((heads, HEAD_DIM, HEAD_DIM), F32), V((heads, 16, HEAD_DIM), F32),
        V((heads, HEAD_DIM + 16, HEAD_DIM), BF16), V((heads, HEAD_DIM + 16, HEAD_DIM), BF16),
        V((heads, HEAD_DIM, HEAD_DIM), BF16), V((heads, HEAD_DIM, HEAD_DIM), BF16),
        V((heads, HEAD_DIM + 16, HEAD_DIM), BF16), V((heads, HEAD_DIM + 16, HEAD_DIM), BF16),
        V((tokens, width), BF16), V((2, G, R, D), BF16), V((G, R, D), BF16),
        V((max(G - 1, 1), R, D), BF16), V((max(G - 1, 1), R, D), BF16),
        pltpu.SemaphoreType.DMA((9,)),
        pltpu.SemaphoreType.DMA((POOL + 3,)),
        pltpu.SemaphoreType.DMA((copies,)),
    ]
    return pl.pallas_call(
        functools.partial(kernel, E, T, cap, near, slots, each, make_plan()),
        out_shape=(
            pltpu.VMEM((R, D), BF16),
            pltpu.VMEM((ntok, Dl), BF16),
        ),
        in_specs=(
            [anyspace] * 4 + [vm, anyspace, vm, anyspace] + [vm] * 4 + [anyspace] * 3
        ),
        out_specs=(vm, vm),
        scratch_shapes=scratch,
        compiler_params=pltpu.CompilerParams(
            collective_id=0, has_side_effects=True, vmem_limit_bytes=60 * 1024 * 1024
        ),
    )(
        q, f, v, o, gap[None], extra, hscale[None], mixw, tok, escale[None],
        routes.T, scores.T, gate[0], up[0], down[0],
    )


def solution(mesh):
    E, T = mesh.shape["ep"], mesh.shape["tp"]
    return jax.shard_map(
        functools.partial(body, E, T),
        mesh=mesh,
        in_specs=(
            P("ep", "tp"),
            P("ep", "tp"),
            P("ep", "tp"),
            P("ep", "tp"),
            P("tp"),
            P("ep", "tp"),
            P("tp"),
            P("tp", None),
            P("ep", None),
            P(),
            P("ep", None),
            P("ep", None),
            P("ep", None, "tp"),
            P("ep", None, "tp"),
            P("ep", None, "tp"),
        ),
        out_specs=(P(("ep", "tp"), None), P("ep", "tp")),
        check_vma=False,
    )
```

```python
import functools

import jax
import jax.numpy as jnp
from jax import lax
from jax.experimental import pallas as pl
from jax.experimental.pallas import tpu as pltpu
from jax.sharding import PartitionSpec as P

HEAD_DIM = 128
CHUNK = 64
POOL = 24
MESH = pl.DeviceIdType.MESH
F32 = jnp.float32
BF16 = jnp.bfloat16


def flip(i, k):
    b = 1
    while b <= k:
        if k & b:
            i = i + b - 2 * b * lax.rem(lax.div(i, b), 2)
        b *= 2
    return i


def kernel(
    E, T, cap, near, slots, each, plan,
    q_hbm, f_hbm, v_hbm, o_hbm, gap_ref, extra_hbm, hscale_ref,
    mixw_hbm, tok_ref, escale_ref, routes_ref, scores_ref,
    gate_hbm, up_hbm, down_hbm,
    mix_out, exp_out,
    q_ref, f_ref, v_ref, o_ref, extra_ref,
    gate, up, down, mixw,
    ncols, dmat, wmat, outgoing, nearout, feats, hidden, part, precv, xsend, xrecv, fin, ret,
    qs, ks, run, qg, rec, ist, idec, est, bst, bdec, psum, pdec, ksend, krecv, csend, crecv, tsend, trecv,
    mhid, mpart, mprecv, mxsend, mxrecv,
    wsem, send_sem, recv_sem,
):
    me = lax.axis_index("ep")
    t = lax.axis_index("tp")
    G = T // 2
    g, c = lax.div(t, 2), lax.rem(t, 2)
    oc = 1 - c
    tokens, width = q_ref.shape
    heads = width // HEAD_DIM
    Dl = outgoing.shape[1]
    FFl = hidden.shape[1]

    loads = [
        pltpu.make_async_copy(src, dst, wsem.at[i])
        for i, (src, dst) in enumerate(
            (
                (f_hbm, f_ref), (extra_hbm, extra_ref), (q_hbm, q_ref), (v_hbm, v_ref),
                (gate_hbm, gate), (up_hbm, up), (down_hbm, down),
                (o_hbm, o_ref), (mixw_hbm, mixw),
            )
        )
    ]

    barrier = pltpu.get_barrier_semaphore()
    for k in range(1, E):
        pl.semaphore_signal(barrier, inc=1, device_id=(flip(me, k), t), device_id_type=MESH)
    pl.semaphore_signal(barrier, inc=1, device_id=(me, 2 * g + oc), device_id_type=MESH)
    for j in range(1, G):
        pl.semaphore_signal(
            barrier, inc=1, device_id=(me, 2 * flip(g, j) + c), device_id_type=MESH
        )

    for load in loads:
        load.start()

    used = [0]
    sent = []
    idle = list(range(POOL))

    def send_slot():
        if idle:
            return idle.pop(0)
        copy, slot = sent.pop(0)
        copy.wait_send()
        return slot

    def remote(src, dst, device, held=None):
        recv, slot = used[0], send_slot() if held is None else held
        used[0] += 1
        copy = pltpu.make_async_remote_copy(
            src_ref=src, dst_ref=dst, send_sem=send_sem.at[slot], recv_sem=recv_sem.at[recv],
            device_id=device, device_id_type=MESH,
        )
        return copy, slot

    def launch(made):
        made[0].start()
        sent.append(made)
        return made[0]

    partner = (me, 2 * g + oc)

    x = tok_ref[...].astype(F32)
    mean = jnp.mean(x, axis=-1, keepdims=True)
    centred = x - mean
    inv = lax.rsqrt(jnp.mean(centred * centred, axis=-1, keepdims=True) + 1e-05)

    def normed(cols):
        return ((tok_ref[:, cols].astype(F32) - mean) * inv * escale_ref[:, cols]).astype(BF16)

    ntok = tok_ref.shape[0]
    ek = lax.broadcasted_iota(jnp.int32, (E, ntok), 0) ^ me
    first, second = routes_ref[0:1, :] == ek, routes_ref[1:2, :] == ek
    named = jnp.where(first | second, 1.0, 0.0)
    earlier = jnp.where(
        lax.broadcasted_iota(jnp.int32, (ntok, ntok), 0)
        < lax.broadcasted_iota(jnp.int32, (ntok, ntok), 1), 1.0, 0.0
    ).astype(BF16)
    position = jnp.dot(named.astype(BF16), earlier, preferred_element_type=F32)
    place = jnp.where(first | second, position, -1.0).astype(jnp.int32)
    rows = lax.broadcasted_iota(jnp.int32, (cap, ntok), 0)

    z = lax.div(me, 2)
    Z = E // 2
    swap = E == 8
    inner = lax.rem(z + lax.div(z, 2), 2) if swap else 0

    def by_side(a, b):
        return a + inner * (b - a)

    def peer(a, b):
        return flip(me, a) if a == b else by_side(flip(me, a), flip(me, b))

    def row_of(table, i):
        a, b = (to[i] for to in slots["to"])
        outside, inside = table[a:a + 1, :], table[b:b + 1, :]
        return outside if a == b else jnp.where(inner == 1, inside, outside)

    def cross(i):
        return (i - near) % 2 if swap else 0

    def choose(i):
        dmat[i * cap:(i + 1) * cap, :] = jnp.where(rows == row_of(place, i), 1.0, 0.0).astype(BF16)

    for i in range(near, E):
        choose(i)
    own = normed(pl.ds(pl.multiple_of(t * Dl, 128), Dl))
    outgoing[...] = jnp.dot(
        dmat[near * cap:, :], own, preferred_element_type=F32
    ).astype(BF16)

    dispatch = {}

    far_base, back_base = used[0] - near, used[0] + E - near - 1
    used[0] += E - near + E - 1

    def placed(src, dst, position, device, slot, base):
        block = pl.ds(pl.multiple_of(position * cap, 16), cap)
        copy = pltpu.make_async_remote_copy(
            src_ref=src, dst_ref=dst(block), send_sem=send_sem.at[slot],
            recv_sem=recv_sem.at[base + position], device_id=device, device_id_type=MESH,
        )
        return copy, slot

    def far_block(block):
        return feats.at[c, g, block]

    def ret_block(block):
        return ret.at[block]

    def send_far(i):
        a, b = (to[i] for to in slots["to"])
        to = near + 2 * inner + (i - near) // 2 if swap else i
        src = outgoing.at[pl.ds((i - near) * cap, cap)]
        launch(placed(src, far_block, to, (peer(a, b), t), send_slot(), far_base))

    def far_arrived(i):
        src = outgoing.at[pl.ds((i - near) * cap, cap)]
        placed(src, far_block, i, partner, 0, far_base)[0].wait_recv()

    def send_back(i):
        a, b = (source[i] for source in slots["from"])
        to = near + inner + 2 * cross(i) if swap and i >= near else i
        src = fin.at[pl.ds(i * cap, cap)]
        launch(placed(src, ret_block, to, (peer(a, b), t), send_slot(), back_base))

    def back_arrived(i):
        placed(fin.at[pl.ds(i * cap, cap)], ret_block, i, partner, 0, back_base)[0].wait_recv()

    def send_near(i):
        dispatch[i] = launch(remote(
            nearout.at[:, pl.ds((i - 1) * cap, cap)],
            feats.at[c, :, pl.ds(i * cap, cap)], (flip(me, i), t),
        ))

    pl.semaphore_wait(barrier, E - 1 + 1 + G - 1)

    def far_out(p):
        for i in range(p * each, (p + 1) * each):
            send_far(i)

    def near_out(p):
        for i in range(max(1, p * each), (p + 1) * each):
            send_near(i)

    def near_prepare():
        for i in range(near):
            choose(i)
        for d in range(T):
            ncols[d % 2, d // 2] = normed(slice(d * Dl, (d + 1) * Dl))
        for j in range(G):
            nearout[j] = jnp.dot(
                dmat[cap:near * cap, :], ncols[c, j], preferred_element_type=F32
            ).astype(BF16)

    def local_features():
        for d in range(T):
            feats[d % 2, d // 2, 0:cap, :] = jnp.dot(
                dmat[0:cap, :], ncols[d % 2, d // 2], preferred_element_type=F32
            ).astype(BF16)

    r_i = lax.broadcasted_iota(jnp.int32, (CHUNK, CHUNK), 0)
    c_i = lax.broadcasted_iota(jnp.int32, (CHUNK, CHUNK), 1)
    causal = r_i >= c_i
    nchunks = tokens // CHUNK

    def head_local(h, _):
        lanes = pl.ds(pl.multiple_of(h * HEAD_DIM, HEAD_DIM), HEAD_DIM)
        state = jnp.zeros((HEAD_DIM, HEAD_DIM), F32)
        before = jnp.zeros((1, HEAD_DIM), F32)
        for n in range(nchunks):
            rs = slice(n * CHUNK, (n + 1) * CHUNK)
            r = run[rs, lanes]
            total = r[CHUNK - 1:CHUNK, :]
            qd = qs[rs, lanes] * jnp.exp(r)
            key = ks[rs, lanes]
            kd = (key * jnp.exp(-r)).astype(BF16)
            kst = (key * jnp.exp(total - r)).astype(BF16)
            val = v_ref[rs, lanes]
            qd_b = qd.astype(BF16)
            scores = lax.dot_general(
                qd_b, kd, (((1,), (1,)), ((), ())), preferred_element_type=F32
            )
            scores = jnp.where(causal, scores, 0.0).astype(BF16)
            out = jnp.dot(scores, val, preferred_element_type=F32)
            if n:
                out += lax.dot_general(
                    qd_b, state.astype(BF16), (((1,), (1,)), ((), ())),
                    preferred_element_type=F32,
                )
            rec[rs, lanes] = out
            qg[rs, lanes] = (qd * jnp.exp(before)).astype(BF16)
            state = state * jnp.exp(total) + lax.dot_general(
                val, kst, (((0,), (0,)), ((), ())), preferred_element_type=F32
            )
            before = before + total
        ist[h] = state
        idec[h] = jnp.broadcast_to(jnp.exp(before), (16, HEAD_DIM))
        return 0

    odd = lax.rem(me, 2) == 1
    pair = remote(ksend, krecv, (flip(me, 1), t))
    scan = E == 8
    if scan:
        climb = remote(tsend, trecv, (lax.rem(me + 2, E), t), POOL)[0]
        hand = [
            remote(csend, crecv, (lax.rem(me + 2 + 2 * i, E), t), POOL + 1 + i)[0]
            for i in range(2)
        ]
    chain = None
    if Z > 1 and not scan:
        chain = remote(csend, crecv, (lax.rem(me + 2, E), t), POOL)[0]

    def recurrence():
        for load in loads[:4]:
            load.wait()
        closing = gap_ref[...] * jax.nn.sigmoid(-f_ref[...].astype(F32))
        ks[...] = closing
        logd = jnp.log1p(-closing) + extra_ref[...]
        qs[...] = jax.nn.silu(q_ref[...].astype(F32))
        tri = jnp.where(causal, 1.0, 0.0).astype(F32)
        for n in range(nchunks):
            run[n * CHUNK:(n + 1) * CHUNK, :] = jnp.dot(
                tri, logd[n * CHUNK:(n + 1) * CHUNK, :], precision=lax.Precision.HIGHEST,
                preferred_element_type=F32,
            )

        lax.fori_loop(0, heads, head_local, 0)
        ksend[:, 0:HEAD_DIM, :] = ist[...].astype(BF16)
        ksend[:, HEAD_DIM:, :] = idec[...].astype(BF16)
        launch(pair)

    def pair_end():
        pair[0].wait_recv()
        s = krecv[:, 0:HEAD_DIM, :].astype(F32)
        d = krecv[:, HEAD_DIM:, :].astype(F32)
        bst[...] = jnp.where(odd, s, 0.0)
        bdec[...] = jnp.where(odd, d, 1.0)
        psum[...] = jnp.where(
            odd, idec[:, 0:1, :] * s + ist[...], d[:, 0:1, :] * ist[...] + s
        )
        pdec[...] = idec[...] * d

    def carry_in(carry):
        est[...] = bdec[:, 0:1, :] * carry + bst[...]

    def scan_step(i):
        if i == 0:
            @pl.when(lax.rem(z, 2) == 0)
            def _():
                est[...] = bst[...]
                tsend[:, 0:HEAD_DIM, :] = psum[...].astype(BF16)
                tsend[:, HEAD_DIM:, :] = pdec[...].astype(BF16)
                climb.start()
        elif i == 1:
            @pl.when(lax.rem(z, 2) == 1)
            def _():
                climb.wait_recv()

            @pl.when(z == 1)
            def _():
                carry = trecv[:, 0:HEAD_DIM, :].astype(F32)
                carry_in(carry)
                csend[...] = (pdec[:, 0:1, :] * carry + psum[...]).astype(BF16)
                hand[0].start()
                hand[1].start()
        elif i == 2:
            @pl.when(z == 2)
            def _():
                hand[0].wait_recv()
                carry_in(crecv[...].astype(F32))

            @pl.when(z == 3)
            def _():
                hand[1].wait_recv()
                decay = trecv[:, HEAD_DIM:HEAD_DIM + 1, :].astype(F32)
                carry_in(decay * crecv[...].astype(F32) + trecv[:, 0:HEAD_DIM, :].astype(F32))

    def chain_step(i):
        if scan:
            scan_step(i)
            return

        @pl.when(z == i)
        def _():
            if i:
                chain.wait_recv()
                carry = crecv[...].astype(F32)
                est[...] = bdec[:, 0:1, :] * carry + bst[...]
                if i + 1 < Z:
                    csend[...] = (pdec[:, 0:1, :] * carry + psum[...]).astype(BF16)
            else:
                est[...] = bst[...]
                if i + 1 < Z:
                    csend[...] = psum[...].astype(BF16)
            if i + 1 < Z:
                chain.start()

    def weigh():
        w0 = jax.nn.sigmoid(scores_ref[0:1, :] - scores_ref[1:2, :])
        weight = jnp.where(first, w0, jnp.where(second, 1.0 - w0, 0.0))
        for i in range(E):
            wmat[i * cap:(i + 1) * cap, :] = jnp.where(
                rows == row_of(place, i), row_of(weight, i), 0.0
            ).astype(BF16)

    ag_partner, ag_cross, rs_partner, rs_cross = {}, {}, {}, {}

    def unit(p):
        return p * each, each

    def piece_rows(p):
        return pl.ds(p * each * cap, each * cap)

    def gather_start(p):
        a, n = unit(p)
        lo = max(a, 1)
        if lo == a + n:
            return
        for i in range(lo, a + n):
            dispatch[i].wait_recv() if i < near else far_arrived(i)
        if a < near:
            rr = pl.ds(lo * cap, (a + n - lo) * cap)
            ag_partner[p, 0] = launch(remote(feats.at[c, :, rr], feats.at[c, :, rr], partner))
            return
        rr = piece_rows(p)
        for j in range(1, G):
            ag_cross[p, j] = launch(
                remote(feats.at[c, g, rr], feats.at[c, g, rr], (me, 2 * flip(g, j) + c))
            )
        ag_partner[p, 0] = launch(remote(feats.at[c, g, rr], feats.at[c, g, rr], partner))

    def gather_relay(p):
        rr = piece_rows(p)
        for j in range(1, G):
            ag_cross[p, j].wait_recv()
            gj = flip(g, j)
            ag_partner[p, j] = launch(remote(feats.at[c, gj, rr], feats.at[c, gj, rr], partner))

    def gather_end(p):
        for j in range(G):
            if (p, j) in ag_partner:
                ag_partner[p, j].wait_recv()

    tile = min(256, FFl)

    def experts(*units):
        if not rs_partner:
            for load in loads[4:7]:
                load.wait()
        for p in units:
            gather_end(p)
        n = len(units) * each
        rs = slice(units[0] * each * cap, (units[-1] + 1) * each * cap)
        for i in range(FFl // tile):
            cc = slice(i * tile, (i + 1) * tile)
            ga = jnp.zeros((n * cap, tile), F32)
            ua = jnp.zeros((n * cap, tile), F32)
            for d in range(T):
                xs = feats[d % 2, d // 2, rs, :]
                ga += jnp.dot(xs, gate[d * Dl:(d + 1) * Dl, cc], preferred_element_type=F32)
                ua += jnp.dot(xs, up[d * Dl:(d + 1) * Dl, cc], preferred_element_type=F32)
            hidden[rs, cc] = (jax.nn.silu(ga) * ua).astype(BF16)

        def down_group(cls, gg):
            ff = pl.ds(pl.multiple_of((2 * gg + cls) * Dl, 128), Dl)
            part[cls, gg, rs, :] = lax.dot_general(
                hidden[rs, :], down[ff, :], (((1,), (1,)), ((), ())),
                preferred_element_type=F32,
            ).astype(BF16)

        for gg in range(G):
            down_group(oc, gg)
        for p in units:
            rr = piece_rows(p)
            rs_partner[p] = launch(remote(part.at[oc, :, rr], precv.at[:, rr], partner))
        for gg in range(G):
            down_group(c, gg)

    def scatter_cross(p):
        a, n = unit(p)
        rs = slice(a * cap, (a + n) * cap)
        rr = piece_rows(p)
        rs_partner[p].wait_recv()
        for j in range(1, G):
            gj = flip(g, j)
            xsend[j - 1, rs, :] = (
                part[c, gj, rs, :].astype(F32) + precv[gj, rs, :].astype(F32)
            ).astype(BF16)
            rs_cross[p, j] = launch(
                remote(xsend.at[j - 1, rr], xrecv.at[j - 1, rr], (me, 2 * gj + c))
            )

    def give_back(p):
        a, n = unit(p)
        rs = slice(a * cap, (a + n) * cap)
        total = part[c, g, rs, :].astype(F32) + precv[g, rs, :].astype(F32)
        for j in range(1, G):
            rs_cross[p, j].wait_recv()
            total += xrecv[j - 1, rs, :].astype(F32)
        fin[rs, :] = total.astype(BF16)
        for i in range(max(a, 1), a + n):
            send_back(i)
        if a == 0:
            ret[0:cap, :] = fin[0:cap, :]

    def mixer_end():
        for load in loads[7:]:
            load.wait()
        for h in range(heads):
            lanes = slice(h * HEAD_DIM, (h + 1) * HEAD_DIM)
            r = rec[:, lanes] + lax.dot_general(
                qg[:, lanes], est[h].astype(BF16), (((1,), (1,)), ((), ())),
                preferred_element_type=F32,
            )
            r = r * lax.rsqrt(jnp.mean(r * r, axis=-1, keepdims=True) + 1e-06)
            mhid[:, lanes] = (
                r * hscale_ref[:, lanes] * jax.nn.silu(o_ref[:, lanes].astype(F32))
            ).astype(BF16)
        R = mix_out.shape[0]
        wide = mixw.shape[1]
        step = min(512, wide)

        def one(i, _):
            cc = pl.ds(pl.multiple_of(i * step, step), step)
            y = jnp.dot(mhid[...], mixw[:, cc], preferred_element_type=F32).astype(BF16)
            for d in range(T):
                mpart[d % 2, d // 2, :, cc] = y[d * R:(d + 1) * R, :]
            return 0

        lax.fori_loop(0, wide // step, one, 0)
        rs_partner["m"] = launch(remote(mpart.at[oc], mprecv, partner))

    def mixer_cross():
        rs_partner["m"].wait_recv()
        for j in range(1, G):
            gj = flip(g, j)
            mxsend[j - 1] = (mpart[c, gj].astype(F32) + mprecv[gj].astype(F32)).astype(BF16)
            rs_cross["m", j] = launch(
                remote(mxsend.at[j - 1], mxrecv.at[j - 1], (me, 2 * gj + c))
            )

    def mixer_out():
        total = mpart[c, g].astype(F32) + mprecv[g].astype(F32)
        for j in range(1, G):
            rs_cross["m", j].wait_recv()
            total += mxrecv[j - 1].astype(F32)
        mix_out[...] = total.astype(BF16)

    def chain_rest(i):
        for i in range(i, Z):
            chain_step(i)

    steps = {
        "f": far_out, "n": near_out, "p": near_prepare, "l": local_features, "h": recurrence,
        "a": gather_start, "b": gather_relay, "c": experts, "d": scatter_cross, "e": give_back,
        "pair": pair_end, "chain": chain_step, "chains": chain_rest,
        "w": weigh, "mc": mixer_end, "md": mixer_cross, "me": mixer_out,
    }
    for step in plan:
        steps[step[0]](*step[1:])
    assert used[0] <= recv_sem.shape[0]
    total = 0.0
    for lo, hi in ((0, near), (near, E)):
        for i in range(max(lo, 1), hi):
            back_arrived(i)
        span = slice(lo * cap, hi * cap)
        total += lax.dot_general(
            wmat[span, :], ret[span, :], (((0,), (0,)), ((), ())), preferred_element_type=F32
        )
    exp_out[...] = total.astype(BF16)
    for copy, _ in sent:
        copy.wait_send()
    if scan:
        @pl.when(lax.rem(z, 2) == 0)
        def _():
            climb.wait_send()

        @pl.when(z == 1)
        def _():
            hand[0].wait_send()
            hand[1].wait_send()

    if chain is not None:
        @pl.when(me + 2 < E)
        def _():
            chain.wait_send()


STEPS = (
    "f 4", "f 5", "p", "n 1", "f 6", "f 7", "h", "n 2", "l", "c 0", "a 4", "d 0",
    "a 1", "c 1", "a 5", "b 4", "pair", "chain 0", "n 3", "d 1", "c 4", "b 5", "a 2", "a 6",
    "d 4", "a 7",
    "c 5", "chain 1", "d 5", "a 3", "e 0", "e 1", "c 2 3", "d 2", "d 3", "e 4", "chain 2", "b 6",
    "b 7", "c 6 7", "d 6", "d 7", "e 5", "chains 3", "mc", "e 2", "e 6", "md", "e 7", "w",
    "e 3", "me",
)


def make_plan():
    return [(s[0], *(int(i) for i in s[1:])) for s in map(str.split, STEPS)]


def body(E, T, q, f, v, o, gap, extra, hscale, mixw, tok, escale, routes, scores, gate, up, down):
    tokens, width = q.shape
    ntok, D = tok.shape
    heads = width // HEAD_DIM
    G = T // 2
    cap = -(-(3 * ntok // E) // 16) * 16
    S = E * cap
    Dl = D // T
    FFl = gate.shape[2]
    R = tokens // T
    near = E // 2
    each = E // 8
    close, far = list(range(near)), list(range(near, E))
    plain = (close + far, close + far)
    slots = {"to": plain, "from": plain}
    if E == 8:
        slots["to"] = (close + [6, 4, 7, 5], close + [4, 6, 5, 7])
        slots["from"] = (close + [6, 7, 4, 5], close + [4, 5, 6, 7])
    copies = 2 * E - near - 1 + near - 1 + 8 + 4 * (2 * G - 1) + 9 * G
    vm = pl.BlockSpec(memory_space=pltpu.VMEM)
    anyspace = pl.BlockSpec(memory_space=pl.ANY)
    V = pltpu.VMEM
    scratch = [
        V(q.shape, BF16), V(q.shape, BF16), V(q.shape, BF16), V(q.shape, BF16), V(q.shape, F32),
        V((D, FFl), BF16), V((D, FFl), BF16), V((D, FFl), BF16), V(mixw.shape, BF16),
        V((2, G, ntok, Dl), BF16), V((S, ntok), BF16), V((S, ntok), BF16),
        V(((E - near) * cap, Dl), BF16), V((G, (near - 1) * cap, Dl), BF16),
        V((2, G, S, Dl), BF16), V((S, FFl), BF16), V((2, G, S, Dl), BF16), V((G, S, Dl), BF16),
        V((max(G - 1, 1), S, Dl), BF16), V((max(G - 1, 1), S, Dl), BF16),
        V((S, Dl), BF16), V((S, Dl), BF16),
        V((tokens, width), F32), V((tokens, width), F32), V((tokens, width), F32),
        V((tokens, width), BF16), V((tokens, width), F32),
        V((heads, HEAD_DIM, HEAD_DIM), F32), V((heads, 16, HEAD_DIM), F32),
        V((heads, HEAD_DIM, HEAD_DIM), F32),
        V((heads, HEAD_DIM, HEAD_DIM), F32), V((heads, 16, HEAD_DIM), F32),
        V((heads, HEAD_DIM, HEAD_DIM), F32), V((heads, 16, HEAD_DIM), F32),
        V((heads, HEAD_DIM + 16, HEAD_DIM), BF16), V((heads, HEAD_DIM + 16, HEAD_DIM), BF16),
        V((heads, HEAD_DIM, HEAD_DIM), BF16), V((heads, HEAD_DIM, HEAD_DIM), BF16),
        V((heads, HEAD_DIM + 16, HEAD_DIM), BF16), V((heads, HEAD_DIM + 16, HEAD_DIM), BF16),
        V((tokens, width), BF16), V((2, G, R, D), BF16), V((G, R, D), BF16),
        V((max(G - 1, 1), R, D), BF16), V((max(G - 1, 1), R, D), BF16),
        pltpu.SemaphoreType.DMA((9,)),
        pltpu.SemaphoreType.DMA((POOL + 3,)),
        pltpu.SemaphoreType.DMA((copies,)),
    ]
    return pl.pallas_call(
        functools.partial(kernel, E, T, cap, near, slots, each, make_plan()),
        out_shape=(
            pltpu.VMEM((R, D), BF16),
            pltpu.VMEM((ntok, Dl), BF16),
        ),
        in_specs=(
            [anyspace] * 4 + [vm, anyspace, vm, anyspace] + [vm] * 4 + [anyspace] * 3
        ),
        out_specs=(vm, vm),
        scratch_shapes=scratch,
        compiler_params=pltpu.CompilerParams(
            collective_id=0, has_side_effects=True, vmem_limit_bytes=60 * 1024 * 1024
        ),
    )(
        q, f, v, o, gap[None], extra, hscale[None], mixw, tok, escale[None],
        routes.T, scores.T, gate[0], up[0], down[0],
    )


def solution(mesh):
    E, T = mesh.shape["ep"], mesh.shape["tp"]
    return jax.shard_map(
        functools.partial(body, E, T),
        mesh=mesh,
        in_specs=(
            P("ep", "tp"),
            P("ep", "tp"),
            P("ep", "tp"),
            P("ep", "tp"),
            P("tp"),
            P("ep", "tp"),
            P("tp"),
            P("tp", None),
            P("ep", None),
            P(),
            P("ep", None),
            P("ep", None),
            P("ep", None, "tp"),
            P("ep", None, "tp"),
            P("ep", None, "tp"),
        ),
        out_specs=(P(("ep", "tp"), None), P("ep", "tp")),
        check_vma=False,
    )
```
